32 devices in a mesh: ra: 4 (over y, x), cb: 8 (over z, core).
Axes of the slice: x: 2, y: 2, z: 4, core: 2. Of those that a mesh axis runs over, the one named last changes fastest.
Arguments:
- tokens: bfloat16 [2048, 2048], P('cb', 'ra'), may hold values from -40 to 40
- gain_first: float32 [2048], replicated, may hold values from 0.1 to 1.9
- gate_first: float32 [2048, 5632], P('cb', 'ra'), may hold values from -0.125 to 0.125
- gate_first_scale: float32 [5632], P('ra'), may hold values from 0.5 to 2
- up_first: float32 [2048, 5632], P('cb', 'ra'), may hold values from -0.125 to 0.125
- up_first_scale: float32 [5632], P('ra'), may hold values from 0.5 to 2
- down_first: float32 [5632, 2048], P('ra', 'cb'), may hold values from -0.078125 to 0.078125
- down_first_scale: float32 [2048], replicated, may hold values from 0.5 to 2
- gain_second: float32 [2048], replicated, may hold values from 0.1 to 1.9
- gate_second: float32 [2048, 5632], P('cb', 'ra'), may hold values from -0.125 to 0.125
- gate_second_scale: float32 [5632], P('ra'), may hold values from 0.5 to 2
- up_second: float32 [2048, 5632], P('cb', 'ra'), may hold values from -0.125 to 0.125
- up_second_scale: float32 [5632], P('ra'), may hold values from 0.5 to 2
- down_second: float32 [5632, 2048], P('ra', 'cb'), may hold values from -0.078125 to 0.078125
- down_second_scale: float32 [2048], replicated, may hold values from 0.5 to 2
- gain_last: float32 [2048], replicated, may hold values from 0.1 to 1.9
Outputs:
- mixed: bfloat16 [2048, 2048], P('cb', 'ra')
The draws below stay inside these ranges and needn't reach their ends.
All inputs are finite; a program needn't handle non-finite values.
Results may differ from the reference program's by a relative error of at most 0.025.
Values may be sent and summed in bfloat16 or wider, within the bound.
A program may use at most 64 MiB of HBM per device.

```python
import math
import jax
import jax.numpy as jnp
from jax import lax

D = 2048
FF = 5632
TOK = 2048


def draw_tokens(key, part):
    first_key = jax.random.fold_in(key, 11)
    second_key = jax.random.fold_in(key, 12)
    column = jnp.arange(D, dtype=jnp.float32)
    rising = 10.0 ** (column / D) * jax.random.uniform(first_key, (D,), jnp.float32, 0.6, 1.6)
    values = jnp.clip(jax.random.normal(second_key, (TOK, D), jnp.float32), -4.0, 4.0)
    return jnp.clip(values * rising, -40.0, 40.0).astype(jnp.bfloat16)


def levels(key, extent, shards, least, high):
    loudness, own = 1.0, jax.random.fold_in(key, 6)
    for axis_at, blocks in shards:
        heights = jnp.exp(jax.random.uniform(jax.random.fold_in(own, axis_at), (blocks,), jnp.float32, least / len(shards), high / len(shards)))
        loudness = loudness * jnp.repeat(heights, extent[axis_at] // blocks).reshape([-1 if axis == axis_at else 1 for axis in range(len(extent))])
    return loudness


def centred(key, extent, scale, reach, pieces=(), kind=jnp.bfloat16):
    result = scale * jax.random.normal(key, extent, jnp.float32)
    if pieces:
        result = result * levels(key, extent, pieces, -0.22, 0.18)
    return jnp.clip(result, -reach, reach).astype(kind)


def setup_inputs(seed: int = 0) -> dict:
    keys = jax.random.split(jax.random.key(seed), 17)
    tokens = draw_tokens(jax.random.fold_in(keys[16], 71), 0)
    gain_first = jnp.clip(1.0 + 0.18 * jax.random.normal(keys[1], (D,), jnp.float32), 0.1, 1.9)
    gate_first = centred(keys[2], (D, FF), D ** -0.5, 0.125, ((0, 8), (1, 4)), jnp.float32)
    gate_first_scale = jnp.clip(jnp.exp(math.log(2.0) - 1.3862944 * jax.random.uniform(keys[3], (FF,), jnp.float32) ** levels(keys[3], (FF,), ((0, 4),), -0.2, 0.2)), 0.5, 2.0)
    up_first = centred(keys[4], (D, FF), D ** -0.5, 0.125, ((0, 8), (1, 4)), jnp.float32)
    up_first_scale = jnp.clip(jnp.exp(math.log(2.0) - 1.3862944 * jax.random.uniform(keys[5], (FF,), jnp.float32) ** levels(keys[5], (FF,), ((0, 4),), -0.2, 0.2)), 0.5, 2.0)
    down_first = centred(keys[6], (FF, D), FF ** -0.5, 0.078125, ((0, 4), (1, 8)), jnp.float32)
    down_first_scale = jnp.clip(jnp.exp(jax.random.uniform(keys[7], (D,), jnp.float32, math.log(0.5), math.log(2.0))), 0.5, 2.0)
    gain_second = jnp.clip(1.0 + 0.18 * jax.random.normal(keys[8], (D,), jnp.float32), 0.1, 1.9)
    gate_second = centred(keys[9], (D, FF), D ** -0.5, 0.125, ((0, 8), (1, 4)), jnp.float32)
    gate_second_scale = jnp.clip(jnp.exp(math.log(2.0) - 1.3862944 * jax.random.uniform(keys[10], (FF,), jnp.float32) ** levels(keys[10], (FF,), ((0, 4),), -0.2, 0.2)), 0.5, 2.0)
    up_second = centred(keys[11], (D, FF), D ** -0.5, 0.125, ((0, 8), (1, 4)), jnp.float32)
    up_second_scale = jnp.clip(jnp.exp(math.log(2.0) - 1.3862944 * jax.random.uniform(keys[12], (FF,), jnp.float32) ** levels(keys[12], (FF,), ((0, 4),), -0.2, 0.2)), 0.5, 2.0)
    down_second = centred(keys[13], (FF, D), FF ** -0.5, 0.078125, ((0, 4), (1, 8)), jnp.float32)
    down_second_scale = jnp.clip(jnp.exp(jax.random.uniform(keys[14], (D,), jnp.float32, math.log(0.5), math.log(2.0))), 0.5, 2.0)
    gain_last = jnp.clip(1.0 + 0.18 * jax.random.normal(keys[15], (D,), jnp.float32), 0.1, 1.9)
    return dict(tokens=tokens, gain_first=gain_first, gate_first=gate_first, gate_first_scale=gate_first_scale, up_first=up_first, up_first_scale=up_first_scale, down_first=down_first, down_first_scale=down_first_scale, gain_second=gain_second, gate_second=gate_second, gate_second_scale=gate_second_scale, up_second=up_second, up_second_scale=up_second_scale, down_second=down_second, down_second_scale=down_second_scale, gain_last=gain_last)


def gated_block(values, gain, w_gate, s_gate, w_up, s_up, w_down, s_down):
    meansq = lax.optimization_barrier(jnp.mean(values * values, axis=1, keepdims=True))
    normed = (values * lax.rsqrt(meansq + 1e-06) * gain).astype(jnp.bfloat16)
    gate = jnp.dot(normed, w_gate.astype(jnp.bfloat16), preferred_element_type=jnp.float32) * s_gate
    upper = jnp.dot(normed, w_up.astype(jnp.bfloat16), preferred_element_type=jnp.float32) * s_up
    hidden = (jax.nn.silu(gate) * upper).astype(jnp.bfloat16)
    return jnp.dot(hidden, w_down.astype(jnp.bfloat16), preferred_element_type=jnp.float32) * s_down

def reference(tokens, gain_first, gate_first, gate_first_scale, up_first, up_first_scale, down_first, down_first_scale, gain_second, gate_second, gate_second_scale, up_second, up_second_scale, down_second, down_second_scale, gain_last):
    start = tokens.astype(jnp.float32)
    first = 0.1 * start + 0.5 * gated_block(start, gain_first, gate_first, gate_first_scale, up_first, up_first_scale, down_first, down_first_scale)
    second = 0.1 * first + 0.5 * gated_block(first, gain_second, gate_second, gate_second_scale, up_second, up_second_scale, down_second, down_second_scale)
    meansq = lax.optimization_barrier(jnp.mean(second * second, axis=1, keepdims=True))
    return (second * lax.rsqrt(meansq + 1e-06) * gain_last).astype(jnp.bfloat16)
```

```python
import functools

import jax
import jax.numpy as jnp
from jax import lax
from jax.experimental import pallas as pl
from jax.experimental.pallas import tpu as pltpu
from jax.sharding import PartitionSpec as P

MESH = pl.DeviceIdType.MESH
D = 2048


def own_slice(vector, width):
    return lax.dynamic_slice_in_dim(vector, lax.axis_index("ra") * width, width, 0)


def full_norm(values, gain):
    meansq = jnp.mean(values * values, axis=1, keepdims=True)
    return (values * lax.rsqrt(meansq + 1e-06) * gain).astype(jnp.bfloat16)


def expand(normed, w_gate, s_gate, w_up, s_up, w_down):
    gate = jnp.dot(
        normed,
        lax.all_gather(w_gate.astype(jnp.bfloat16), "cb", axis=0, tiled=True),
        preferred_element_type=jnp.float32,
    )
    upper = jnp.dot(
        normed,
        lax.all_gather(w_up.astype(jnp.bfloat16), "cb", axis=0, tiled=True),
        preferred_element_type=jnp.float32,
    )
    hidden = (jax.nn.silu(gate * s_gate) * (upper * s_up)).astype(jnp.bfloat16)
    return jnp.dot(
        hidden,
        lax.all_gather(w_down.astype(jnp.bfloat16), "cb", axis=1, tiled=True),
        preferred_element_type=jnp.float32,
    )


def reduce_share(partial_value):
    return lax.psum_scatter(
        partial_value.astype(jnp.bfloat16), "ra", scatter_dimension=1, tiled=True
    ).astype(jnp.float32)


def shards(
    tokens,
    gain_first,
    gate_first,
    gate_first_scale,
    up_first,
    up_first_scale,
    down_first,
    down_first_scale,
    gain_second,
    gate_second,
    gate_second_scale,
    up_second,
    up_second_scale,
    down_second,
    down_second_scale,
    gain_last,
):
    width = tokens.shape[1]
    whole_in = lax.all_gather(tokens, "ra", axis=1, tiled=True).astype(jnp.float32)
    normed = full_norm(whole_in, gain_first)
    partial_value = expand(
        normed, gate_first, gate_first_scale, up_first, up_first_scale, down_first
    )
    summed = lax.psum(partial_value.astype(jnp.bfloat16), "ra").astype(jnp.float32)
    first = 0.1 * whole_in + 0.5 * summed * down_first_scale
    first_share = own_slice(first.T, width).T
    normed_next = full_norm(first, gain_second)
    partial_next = expand(
        normed_next, gate_second, gate_second_scale, up_second, up_second_scale, down_second
    )
    second = 0.1 * first_share + 0.5 * reduce_share(partial_next) * own_slice(
        down_second_scale, width
    )
    closing = lax.psum(jnp.sum(second * second, axis=1), "ra")
    return (second * lax.rsqrt(closing / D + 1e-06)[:, None] * own_slice(gain_last, width)).astype(
        jnp.bfloat16
    )


def remote(source, target, sent, received, device):
    return pltpu.make_async_remote_copy(
        src_ref=source,
        dst_ref=target,
        send_sem=sent,
        recv_sem=received,
        device_id=device,
        device_id_type=MESH,
    )


def kernel(chips, *refs):
    (tokens, gain_first, scale_first, gain_second, scale_second, gain_last) = refs[:6]
    scales = refs[6:10]
    weights = refs[10:16]
    out = refs[16]
    stages = refs[17:23]
    (
        sendable,
        whole,
        rows_in,
        normed,
        hidden,
        product,
        given,
        taken,
        passed,
        from_below,
        from_above,
        total,
        first,
        stats,
        last,
        load_sem,
        wz_s,
        wz_r,
        wx_s,
        wx_r,
        wk_s,
        wk_r,
        tx_s,
        tx_r,
        az_s,
        az_r,
        ay_s,
        ay_r,
        ry_s,
        ry_r,
        rz_s,
        rzu_r,
        rzd_r,
        end_s,
        end_r,
    ) = refs[23:]
    count = chips
    half_rows = tokens.shape[0] // 2
    columns = tokens.shape[1]
    width = 4 * columns
    half = width // 2
    units = sendable.shape[1]
    share = units // count
    piece = sendable.shape[2]

    ra, cb = lax.axis_index("ra"), lax.axis_index("cb")
    y, x = lax.div(ra, 2), lax.rem(ra, 2)
    z, k = lax.div(cb, 2), lax.rem(cb, 2)
    far = lax.div(z, 2)

    def device(x_at, y_at, z_at, k_at):
        return (y_at * 2 + x_at, z_at * 2 + k_at)

    on_x = device(1 - x, y, z, k)
    on_y = device(x, 1 - y, z, k)
    on_k = device(x, y, z, 1 - k)
    above = device(x, y, lax.rem(z + 1, count), k)
    below = device(x, y, lax.rem(z + count - 1, count), k)

    def around(d):
        return lax.rem(z + d, count)

    def near(i):
        outer, inner = i // 2, i % 2
        close = z + inner * (1 - 2 * lax.rem(z, 2))
        distant = (2 + inner) - far * (1 + 2 * inner)
        return (1 - outer) * close + outer * distant

    def at_x(x_at):
        return pl.ds(pl.multiple_of(x_at * share, 16), share)

    def at_z(z_at):
        return pl.ds(pl.multiple_of(z_at * share, 16), share)

    def at_column(z_at, k_at):
        return pl.ds(pl.multiple_of(k_at * half + z_at * piece, 128), piece)

    def at_half(h):
        return pl.ds(pl.multiple_of(h * half, 128), half)

    sends = []

    def launch(copy):
        copy.start()
        sends.append((None, copy))

    def launch_if(condition, copy):
        @pl.when(condition)
        def _():
            copy.start()

        sends.append((condition, copy))

    def wait_if(condition, copy):
        @pl.when(condition)
        def _():
            copy.wait_recv()

    barrier = pltpu.get_barrier_semaphore()
    partners = [on_x, on_y, on_k] + [device(x, y, around(d), k) for d in range(1, count)]
    for partner in partners:
        pl.semaphore_signal(barrier, inc=1, device_id=partner, device_id_type=MESH)
    loads = [
        pltpu.make_async_copy(weights[m], stages[m], load_sem.at[m]) for m in range(6)
    ]
    for load in loads:
        load.start()

    def prepare(m):
        loads[m].wait()
        if m % 3 == 2:
            sendable[m] = stages[m][...].astype(jnp.bfloat16)
        else:
            scale = scales[2 * (m // 3) + m % 3]
            for at in range(0, units, 128):
                block = stages[m][:, at : at + 128] * scale[:, at : at + 128]
                sendable[m, at : at + 128, :] = block.T.astype(jnp.bfloat16)
        whole[m, at_x(x), at_column(z, k)] = sendable[m, at_z(z), :]

    def z_copy(m, d):
        return remote(
            sendable.at[m, at_z(around(d)), :],
            whole.at[m, at_x(x), at_column(z, k)],
            wz_s.at[m, d - 1],
            wz_r.at[m, d - 1],
            device(x, y, around(d), k),
        )

    def x_copy(m, d):
        source = whole.at[m, at_x(x), at_column(around(count - d), k)]
        if d == 0:
            return remote(
                sendable.at[m, at_z(z), :],
                whole.at[m, at_x(x), at_column(z, k)],
                wx_s.at[m, 0],
                wx_r.at[m, 0],
                on_x,
            )
        return remote(source, source, wx_s.at[m, d], wx_r.at[m, d], on_x)

    def k_copy(m, side):
        part = whole.at[m, at_x(1 - x if side else x), at_half(k)]
        return remote(part, part, wk_s.at[m, side], wk_r.at[m, side], on_k)

    def send_weights(m):
        for d in range(1, count):
            launch(z_copy(m, d))
        launch(x_copy(m, 0))

    def relay_own(m):
        for d in range(1, count):
            z_copy(m, d).wait_recv()
            launch(x_copy(m, d))
        launch(k_copy(m, 0))

    def relay_other(m):
        for d in range(count):
            x_copy(m, d).wait_recv()
        launch(k_copy(m, 1))

    def await_weights(m):
        for side in range(2):
            k_copy(m, side).wait_recv()

    def gather_z(b, i, up):
        j = near(i)
        part = rows_in.at[b, j, :, at_half(y)]
        return remote(
            part,
            part,
            az_s.at[b, i + (0 if up or i else count)],
            az_r.at[b, j],
            above if up else below,
        )

    def gather_y(b, i):
        part = rows_in.at[b, near(i), :, at_half(y)]
        return remote(part, part, ay_s.at[b, i], ay_r.at[b, i], on_y)

    def gather_step(b, i):
        j = near(i)
        if i == 0:
            launch_if(z < count - 1, gather_z(b, 0, True))
            launch_if(z > 0, gather_z(b, 0, False))
        else:
            gather_z(b, i, True).wait_recv()
            launch_if((j < z) & (z < count - 1), gather_z(b, i, True))
            launch_if((j > z) & (z > 0), gather_z(b, i, False))
        launch(gather_y(b, i))

    def norm_step(b, i):
        j = near(i)
        gather_y(b, i).wait_recv()
        gain = gain_second if b else gain_first
        values = rows_in[b, j].astype(jnp.float32)
        meansq = jnp.sum(values * values, axis=1, keepdims=True) * (1.0 / width)
        values = values * lax.rsqrt(meansq + 1e-06) * gain[...]
        values = values.astype(jnp.bfloat16)
        for block in range(2 * count):
            z_at, k_at = block // 2, block % 2
            normed[j, :, k_at * half + z_at * piece : k_at * half + (z_at + 1) * piece] = (
                values[:, block * piece : (block + 1) * piece]
            )

    def expand_step(b, i):
        j = near(i)
        axes = (((1,), (1,)), ((), ()))
        gate = lax.dot_general(
            normed[j], whole[3 * b], axes, preferred_element_type=jnp.float32
        )
        upper = lax.dot_general(
            normed[j], whole[3 * b + 1], axes, preferred_element_type=jnp.float32
        )
        hidden[j] = (gate / (1.0 + jnp.exp(-gate)) * upper).astype(jnp.bfloat16)

    def reduce_y(b, i):
        j = near(i)
        return remote(given.at[b, j], taken.at[b, j], ry_s.at[b, i], ry_r.at[b, i], on_y)

    def contract_step(b, i):
        j = near(i)
        for k_at in range(2):
            part = jnp.dot(
                hidden[j],
                whole[3 * b + 2, :, k_at * half : (k_at + 1) * half],
                preferred_element_type=jnp.float32,
            )
            for z_at in range(count):
                block = 2 * z_at + k_at
                product[j, :, block * piece : (block + 1) * piece] = part[
                    :, z_at * piece : (z_at + 1) * piece
                ]
        given[b, j] = product[j, :, at_half(1 - y)].astype(jnp.bfloat16)
        reduce_y(b, i).start()

    def reduce_z(b, i, up):
        j = near(i)
        if up:
            return remote(passed.at[b, j], from_below.at[b, j], rz_s.at[b, i], rzu_r.at[b, j], above)
        return remote(passed.at[b, j], from_above.at[b, j], rz_s.at[b, i], rzd_r.at[b, j], below)

    def reduce_step(b, i):
        j = near(i)
        reduce_y(b, i).wait_recv()
        total[...] = product[j, :, at_half(y)] + taken[b, j].astype(jnp.float32)
        rises = (j >= z) & (z > 0)
        falls = (j <= z) & (z < count - 1)

        @pl.when(rises)
        def _():
            reduce_z(b, i, True).wait_recv()
            total[...] += from_below[b, j].astype(jnp.float32)

        @pl.when(falls)
        def _():
            reduce_z(b, i, False).wait_recv()
            total[...] += from_above[b, j].astype(jnp.float32)

        if i:
            passed[b, j] = total[...].astype(jnp.bfloat16)
            launch_if(j > z, reduce_z(b, i, True))
            launch_if(j < z, reduce_z(b, i, False))

    prepare(0)
    pl.semaphore_wait(barrier, len(partners))

    mine = pl.ds(pl.multiple_of(x * half_rows, 16), half_rows)
    theirs = pl.ds(pl.multiple_of((1 - x) * half_rows, 16), half_rows)
    own_columns = pl.ds(pl.multiple_of(ra * columns, 128), columns)
    token_copy = remote(
        tokens.at[theirs, :],
        rows_in.at[0, z, :, own_columns],
        tx_s.at[0],
        tx_r.at[0],
        on_x,
    )
    launch(token_copy)
    rows_in[0, z, :, own_columns] = tokens[mine, :]
    prepare(1)
    token_copy.wait_recv()
    gather_step(0, 0)
    send_weights(0)
    send_weights(1)
    prepare(2)
    gather_step(0, 1)
    prepare(3)
    gather_step(0, 2)
    prepare(4)
    gather_step(0, 3)
    send_weights(2)
    prepare(5)
    for i in range(count):
        norm_step(0, i)
    relay_own(0)
    relay_own(1)
    send_weights(3)
    relay_other(0)
    relay_other(1)
    await_weights(0)
    await_weights(1)
    lax.fori_loop(0, count, lambda i, c: (expand_step(0, i), c)[1], 0)
    relay_own(2)
    relay_other(2)
    await_weights(2)
    lax.fori_loop(0, count, lambda i, c: (contract_step(0, count - 1 - i), c)[1], 0)
    reduce_step(0, 3)
    reduce_step(0, 2)
    relay_own(3)
    reduce_step(0, 1)
    send_weights(4)
    reduce_step(0, 0)
    start = rows_in[0, z, :, at_half(y)].astype(jnp.float32)
    first[...] = 0.1 * start + 0.5 * total[...] * scale_first[:, at_half(y)]
    rows_in[1, z, :, at_half(y)] = first[...].astype(jnp.bfloat16)
    gather_step(1, 0)
    relay_other(3)
    gather_step(1, 1)
    gather_step(1, 2)
    gather_step(1, 3)
    send_weights(5)
    relay_own(4)
    relay_other(4)
    for i in range(count):
        norm_step(1, i)
    await_weights(3)
    await_weights(4)
    lax.fori_loop(0, count, lambda i, c: (expand_step(1, i), c)[1], 0)
    relay_own(5)
    relay_other(5)
    await_weights(5)
    lax.fori_loop(0, count, lambda i, c: (contract_step(1, count - 1 - i), c)[1], 0)
    for i in reversed(range(count)):
        reduce_step(1, i)
    second = 0.1 * first[...] + 0.5 * total[...] * scale_second[:, at_half(y)]
    total[...] = second
    squares = jnp.sum(second * second, axis=1, keepdims=True)
    stats[0] = jnp.broadcast_to(squares, stats.shape[1:])
    stat_copy = remote(stats.at[0], stats.at[1], end_s.at[0], end_r.at[0], on_y)
    launch(stat_copy)
    stat_copy.wait_recv()
    squares = squares + stats[1][:, :1]
    mixed = total[...] * lax.rsqrt(squares * (1.0 / width) + 1e-06) * gain_last[:, at_half(y)]
    total[...] = mixed
    other_columns = pl.ds(pl.multiple_of((1 - x) * columns, 128), columns)
    kept_columns = pl.ds(pl.multiple_of(x * columns, 128), columns)
    last[0] = total[:, other_columns].astype(jnp.bfloat16)
    last_copy = remote(last.at[0], last.at[1], end_s.at[1], end_r.at[1], on_x)
    launch(last_copy)
    out[mine, :] = total[:, kept_columns].astype(jnp.bfloat16)
    for b in range(2):
        for i in range(count):
            reduce_y(b, i).wait_send()
    last_copy.wait_recv()
    out[theirs, :] = last[1]
    for condition, copy in sends:
        if condition is None:
            copy.wait_send()
        else:

            @pl.when(condition)
            def _(copy=copy):
                copy.wait_send()


def fused(tokens, *rest):
    (
        gain_first,
        gate_first,
        gate_first_scale,
        up_first,
        up_first_scale,
        down_first,
        down_first_scale,
        gain_second,
        gate_second,
        gate_second_scale,
        up_second,
        up_second_scale,
        down_second,
        down_second_scale,
        gain_last,
    ) = rest
    chips = lax.axis_size("cb") // 2
    rows, columns = tokens.shape
    piece, units = gate_first.shape
    share = units // chips
    width, half_rows = 4 * columns, rows // 2
    half = width // 2

    def row(vector):
        return vector.reshape(1, -1)

    vmem = pl.BlockSpec(memory_space=pltpu.VMEM)
    anywhere = pl.BlockSpec(memory_space=pl.ANY)
    bf16, f32 = jnp.bfloat16, jnp.float32
    dma = pltpu.SemaphoreType.DMA
    stage_shapes = [w.shape for w in (gate_first, up_first, down_first)] * 2
    moved = pltpu.VMEM((2, chips, half_rows, half), bf16)
    scratch = [pltpu.VMEM(shape, f32) for shape in stage_shapes] + [
        pltpu.VMEM((6, units, piece), bf16),
        pltpu.VMEM((6, 2 * share, width), bf16),
        pltpu.VMEM((2, chips, half_rows, width), bf16),
        pltpu.VMEM((chips, half_rows, width), bf16),
        pltpu.VMEM((chips, half_rows, 2 * share), bf16),
        pltpu.VMEM((chips, half_rows, width), f32),
        moved,
        moved,
        moved,
        moved,
        moved,
        pltpu.VMEM((half_rows, half), f32),
        pltpu.VMEM((half_rows, half), f32),
        pltpu.VMEM((2, half_rows, 128), f32),
        pltpu.VMEM((2, half_rows, columns), bf16),
        dma((6,)),
        dma((6, chips - 1)),
        dma((6, chips - 1)),
        dma((6, chips)),
        dma((6, chips)),
        dma((6, 2)),
        dma((6, 2)),
        dma((1,)),
        dma((1,)),
        dma((2, chips + 1)),
        dma((2, chips)),
        dma((2, chips)),
        dma((2, chips)),
        dma((2, chips)),
        dma((2, chips)),
        dma((2, chips)),
        dma((2, chips)),
        dma((2, chips)),
        dma((2,)),
        dma((2,)),
    ]
    return pl.pallas_call(
        functools.partial(kernel, chips),
        out_shape=jax.ShapeDtypeStruct(tokens.shape, bf16),
        in_specs=[vmem] * 10 + [anywhere] * 6,
        out_specs=vmem,
        scratch_shapes=scratch,
        compiler_params=pltpu.CompilerParams(
            collective_id=0, has_side_effects=True, vmem_limit_bytes=62 * 2**20
        ),
    )(
        tokens,
        row(gain_first),
        row(down_first_scale),
        row(gain_second),
        row(down_second_scale),
        row(gain_last),
        row(gate_first_scale),
        row(up_first_scale),
        row(gate_second_scale),
        row(up_second_scale),
        gate_first,
        up_first,
        down_first,
        gate_second,
        up_second,
        down_second,
    )


def plan_for(mesh):
    ra, cb = mesh.shape["ra"], mesh.shape["cb"]

    def run(tokens, *rest):
        units = rest[1].shape[1]
        aligned = units % (cb * 8) == 0 and units % 128 == 0 and tokens.shape[0] % 32 == 0
        if ra == 4 and cb == 8 and aligned:
            return fused(tokens, *rest)
        return shards(tokens, *rest)

    return run


def solution(mesh):
    placed = (
        P("cb", "ra"),
        P(),
        P("cb", "ra"),
        P("ra"),
        P("cb", "ra"),
        P("ra"),
        P("ra", "cb"),
        P(),
        P(),
        P("cb", "ra"),
        P("ra"),
        P("cb", "ra"),
        P("ra"),
        P("ra", "cb"),
        P(),
        P(),
    )
    return jax.shard_map(
        plan_for(mesh), mesh=mesh, in_specs=placed, out_specs=P("cb", "ra"), check_vma=False
    )
```

```python
import functools

import jax
import jax.numpy as jnp
from jax import lax
from jax.experimental import pallas as pl
from jax.experimental.pallas import tpu as pltpu
from jax.sharding import PartitionSpec as P

MESH = pl.DeviceIdType.MESH
PARTS = 2
D = 2048


def own_slice(vector, width):
    return lax.dynamic_slice_in_dim(vector, lax.axis_index("ra") * width, width, 0)


def full_norm(values, gain):
    meansq = jnp.mean(values * values, axis=1, keepdims=True)
    return (values * lax.rsqrt(meansq + 1e-06) * gain).astype(jnp.bfloat16)


def expand(normed, w_gate, s_gate, w_up, s_up, w_down):
    gate = jnp.dot(
        normed,
        lax.all_gather(w_gate.astype(jnp.bfloat16), "cb", axis=0, tiled=True),
        preferred_element_type=jnp.float32,
    )
    upper = jnp.dot(
        normed,
        lax.all_gather(w_up.astype(jnp.bfloat16), "cb", axis=0, tiled=True),
        preferred_element_type=jnp.float32,
    )
    hidden = (jax.nn.silu(gate * s_gate) * (upper * s_up)).astype(jnp.bfloat16)
    return jnp.dot(
        hidden,
        lax.all_gather(w_down.astype(jnp.bfloat16), "cb", axis=1, tiled=True),
        preferred_element_type=jnp.float32,
    )


def reduce_share(partial_value):
    return lax.psum_scatter(
        partial_value.astype(jnp.bfloat16), "ra", scatter_dimension=1, tiled=True
    ).astype(jnp.float32)


def shards(
    tokens,
    gain_first,
    gate_first,
    gate_first_scale,
    up_first,
    up_first_scale,
    down_first,
    down_first_scale,
    gain_second,
    gate_second,
    gate_second_scale,
    up_second,
    up_second_scale,
    down_second,
    down_second_scale,
    gain_last,
):
    width = tokens.shape[1]
    whole_in = lax.all_gather(tokens, "ra", axis=1, tiled=True).astype(jnp.float32)
    normed = full_norm(whole_in, gain_first)
    partial_value = expand(
        normed, gate_first, gate_first_scale, up_first, up_first_scale, down_first
    )
    summed = lax.psum(partial_value.astype(jnp.bfloat16), "ra").astype(jnp.float32)
    first = 0.1 * whole_in + 0.5 * summed * down_first_scale
    first_share = own_slice(first.T, width).T
    normed_next = full_norm(first, gain_second)
    partial_next = expand(
        normed_next, gate_second, gate_second_scale, up_second, up_second_scale, down_second
    )
    second = 0.1 * first_share + 0.5 * reduce_share(partial_next) * own_slice(
        down_second_scale, width
    )
    closing = lax.psum(jnp.sum(second * second, axis=1), "ra")
    return (second * lax.rsqrt(closing / D + 1e-06)[:, None] * own_slice(gain_last, width)).astype(
        jnp.bfloat16
    )


def remote(source, target, sent, received, device):
    return pltpu.make_async_remote_copy(
        src_ref=source,
        dst_ref=target,
        send_sem=sent,
        recv_sem=received,
        device_id=device,
        device_id_type=MESH,
    )


def kernel(chips, *refs):
    (tokens, gain_first, scale_first, gain_second, scale_second, gain_last) = refs[:6]
    scales = refs[6:10]
    weights = refs[10:16]
    out = refs[16]
    stages = refs[17:23]
    (
        sendable,
        whole,
        rows_in,
        normed,
        hidden,
        product,
        given,
        taken,
        passed,
        from_below,
        from_above,
        total,
        first,
        stats,
        last,
        vectors,
        load_sem,
        wz_s,
        wz_r,
        wp_s,
        wp_r,
        wk_s,
        wk_r,
        tx_s,
        tx_r,
        az_s,
        az_r,
        ay_s,
        ay_r,
        ry_s,
        ry_r,
        rz_s,
        rzu_r,
        rzd_r,
        end_s,
        end_r,
    ) = refs[23:]
    count = chips
    half_rows = tokens.shape[0] // 2
    columns = tokens.shape[1]
    width = 4 * columns
    half = width // 2
    units = sendable.shape[1]
    share = units // count
    part_rows = half_rows // PARTS
    piece = sendable.shape[2]

    ra, cb = lax.axis_index("ra"), lax.axis_index("cb")
    y, x = lax.div(ra, 2), lax.rem(ra, 2)
    z, k = lax.div(cb, 2), lax.rem(cb, 2)
    p, q = x + k * (y - x), y + k * (x - y)
    far = lax.div(z, 2)

    def device(x_at, y_at, z_at, k_at):
        return (y_at * 2 + x_at, z_at * 2 + k_at)

    def turned(p_at, q_at):
        return device(p_at + k * (q_at - p_at), q_at + k * (p_at - q_at), z, k)

    on_p, on_q = turned(1 - p, q), turned(p, 1 - q)
    on_k = device(x, y, z, 1 - k)
    to_x, to_y = device(1 - x, y, z, 0), device(x, 1 - y, z, 1)
    above = device(x, y, lax.rem(z + 1, count), k)
    below = device(x, y, lax.rem(z + count - 1, count), k)

    def around(d):
        return lax.rem(z + d, count)

    def near(i):
        outer, inner = i // 2, i % 2
        close = z + inner * (1 - 2 * lax.rem(z, 2))
        distant = (2 + inner) - far * (1 + 2 * inner)
        return (1 - outer) * close + outer * distant

    def natural(block):
        return block if block in (0, 3) else (1 + k if block == 1 else 2 - k)

    def at_share(n):
        return pl.ds(pl.multiple_of(n * share, 16), share)

    def at_column(z_at, k_at):
        return pl.ds(pl.multiple_of(k_at * half + z_at * piece, 128), piece)

    def at_half(h):
        return pl.ds(pl.multiple_of(h * half, 128), half)

    def at_block(n):
        return pl.ds(pl.multiple_of(n * columns, 128), columns)

    sends = []

    def launch(copy):
        copy.start()
        sends.append((None, copy))

    def launch_if(condition, copy):
        @pl.when(condition)
        def _():
            copy.start()

        sends.append((condition, copy))

    barrier = pltpu.get_barrier_semaphore()
    partners = [device(1 - x, y, z, 0), device(1 - x, y, z, 1), device(x, 1 - y, z, 0)]
    partners += [device(x, 1 - y, z, 1), device(1 - x, 1 - y, z, k), on_k]
    partners += [device(x, y, around(d), k) for d in range(1, count)]
    for partner in partners:
        pl.semaphore_signal(barrier, inc=1, device_id=partner, device_id_type=MESH)
    loads = [
        pltpu.make_async_copy(weights[m], stages[m], load_sem.at[m]) for m in range(6)
    ]
    for load in loads:
        load.start()
    for n, vector in enumerate((gain_first, scale_first, gain_second, scale_second, gain_last)):
        for block in range(4):
            vectors[n, :, block * columns : (block + 1) * columns] = vector[
                :, at_block(natural(block))
            ]

    def prepare(m):
        loads[m].wait()
        if m % 3 == 2:
            sendable[m] = stages[m][...].astype(jnp.bfloat16)
        else:
            scale = scales[2 * (m // 3) + m % 3]
            for at in range(0, units, 128):
                block = stages[m][:, at : at + 128] * scale[at : at + 128][None, :]
                sendable[m, at : at + 128, :] = block.T.astype(jnp.bfloat16)
        whole[m, at_share(p), at_column(z, k)] = sendable[m, at_share(z), :]

    def z_copy(m, d):
        return remote(
            sendable.at[m, at_share(around(d)), :],
            whole.at[m, at_share(p), at_column(z, k)],
            wz_s.at[m, d - 1],
            wz_r.at[m, d - 1],
            device(x, y, around(d), k),
        )

    odd = lax.rem(z, 2)
    outgoing = {"across": 2, "beyond": 3 - 2 * odd, "beside": 1 + 2 * odd}
    incoming = {"own": 0, "across": 2, "beyond": 1 + 2 * odd, "beside": 3 - 2 * odd}

    def send_z(m, *steps):
        for step in steps:
            launch(z_copy(m, outgoing[step]))

    def relay(m, *steps):
        for step in steps:
            d = incoming[step]
            place = at_column(around(count - d), k)
            if step != "own":
                z_copy(m, d).wait_recv()
                source = whole.at[m, at_share(p), place]
            else:
                source = sendable.at[m, at_share(z), :]
            remote(
                source, whole.at[m, at_share(x), place], wp_s.at[m, 0], wp_r.at[m], to_x
            ).start()
            remote(
                source, whole.at[m, at_share(y), place], wp_s.at[m, 1], wp_r.at[m], to_y
            ).start()
            remote(
                source, whole.at[m, at_share(q), place], wk_s.at[m], wk_r.at[m], on_k
            ).start()

    def await_weights(m):
        part = whole.at[m, at_share(1 - p), :]
        remote(part, part, wp_s.at[m, 0], wp_r.at[m], on_p).wait_recv()
        part = whole.at[m, at_share(p), at_half(1 - k)]
        remote(part, part, wk_s.at[m], wk_r.at[m], on_k).wait_recv()

    def drain_weights(m):
        part = whole.at[m, at_share(p), at_half(k)]
        remote(part, part, wp_s.at[m, 0], wp_r.at[m], to_x).wait_send()
        remote(part, part, wp_s.at[m, 1], wp_r.at[m], to_y).wait_send()
        remote(part, part, wk_s.at[m], wk_r.at[m], on_k).wait_send()

    def rows_of(h):
        return slice(h * part_rows, (h + 1) * part_rows)

    def gather_z(b, i, h, up):
        j = near(i)
        part = rows_in.at[b, j, rows_of(h), at_half(q)]
        return remote(
            part,
            part,
            az_s.at[b, h, i + (0 if up or i else count)],
            az_r.at[b, h, j],
            above if up else below,
        )

    def gather_q(b, i, h):
        part = rows_in.at[b, near(i), rows_of(h), at_half(q)]
        return remote(part, part, ay_s.at[b, h, i], ay_r.at[b, h, i], on_q)

    def gather_step(b, i, h):
        j = near(i)
        if i == 0:
            launch_if(z < count - 1, gather_z(b, 0, h, True))
            launch_if(z > 0, gather_z(b, 0, h, False))
        else:
            gather_z(b, i, h, True).wait_recv()
            launch_if((j < z) & (z < count - 1), gather_z(b, i, h, True))
            launch_if((j > z) & (z > 0), gather_z(b, i, h, False))
        launch(gather_q(b, i, h))

    def norm_step(b, i):
        j = near(i)
        for h in range(PARTS):
            gather_q(b, i, h).wait_recv()
        values = rows_in[b, j].astype(jnp.float32)
        meansq = jnp.sum(values * values, axis=1, keepdims=True) * (1.0 / width)
        values = values * lax.rsqrt(meansq + 1e-06) * vectors[2 * b]
        values = values.astype(jnp.bfloat16)
        rows = slice(i * half_rows, (i + 1) * half_rows)
        for block in range(4):
            for side in range(2):
                at = block * columns + side * piece
                normed[rows, at_column(natural(block), side)] = values[:, at : at + piece]

    def expand_step(b, pair):
        axes = (((1,), (1,)), ((), ()))
        rows = pl.ds(pl.multiple_of(pair * 2 * half_rows, 16), 2 * half_rows)
        gate = lax.dot_general(
            normed[rows, :], whole[3 * b], axes, preferred_element_type=jnp.float32
        )
        upper = lax.dot_general(
            normed[rows, :], whole[3 * b + 1], axes, preferred_element_type=jnp.float32
        )
        hidden[rows, :] = (gate / (1.0 + jnp.exp(-gate)) * upper).astype(jnp.bfloat16)

    def reduce_q(b, i, h):
        j = near(i)
        return remote(
            given.at[b, j, rows_of(h)],
            taken.at[b, j, rows_of(h)],
            ry_s.at[b, h, i],
            ry_r.at[b, h, i],
            on_q,
        )

    def contract_step(b, i):
        j = near(i)
        rows = pl.ds(pl.multiple_of(i * half_rows, 16), half_rows)
        for side in range(2):
            part = jnp.dot(
                hidden[rows, :],
                whole[3 * b + 2, :, side * half : (side + 1) * half],
                preferred_element_type=jnp.float32,
            )
            for block in range(4):
                at = pl.multiple_of(natural(block) * columns + side * piece, 128)
                product[j, :, pl.ds(at, piece)] = part[:, block * piece : (block + 1) * piece]
        given[b, j] = product[j, :, at_half(1 - q)].astype(jnp.bfloat16)
        for h in range(PARTS):
            reduce_q(b, i, h).start()

    def reduce_z(b, i, h, up):
        j = near(i)
        landing, arrived, target = (
            (from_below, rzu_r, above) if up else (from_above, rzd_r, below)
        )
        return remote(
            passed.at[b, j, rows_of(h)],
            landing.at[b, j, rows_of(h)],
            rz_s.at[b, h, i],
            arrived.at[b, h, j],
            target,
        )

    def reduce_step(b, i, h):
        j = near(i)
        rows = rows_of(h)
        reduce_q(b, i, h).wait_recv()
        total[rows] = product[j, rows, at_half(q)] + taken[b, j, rows].astype(jnp.float32)
        rises = (j >= z) & (z > 0)
        falls = (j <= z) & (z < count - 1)

        @pl.when(rises)
        def _():
            reduce_z(b, i, h, True).wait_recv()
            total[rows] += from_below[b, j, rows].astype(jnp.float32)

        @pl.when(falls)
        def _():
            reduce_z(b, i, h, False).wait_recv()
            total[rows] += from_above[b, j, rows].astype(jnp.float32)

        if i:
            passed[b, j, rows] = total[rows].astype(jnp.bfloat16)
            launch_if(j > z, reduce_z(b, i, h, True))
            launch_if(j < z, reduce_z(b, i, h, False))

    def restart(h):
        rows = rows_of(h)
        start = rows_in[0, z, rows, at_half(q)].astype(jnp.float32)
        first[rows] = 0.1 * start + 0.5 * total[rows] * vectors[1, :, at_half(q)]
        rows_in[1, z, rows, at_half(q)] = first[rows].astype(jnp.bfloat16)

    prepare(0)
    pl.semaphore_wait(barrier, len(partners))

    mine = pl.ds(pl.multiple_of(p * half_rows, 16), half_rows)
    theirs = pl.ds(pl.multiple_of((1 - p) * half_rows, 16), half_rows)
    own_columns = at_block(2 * q + p)
    token_copy = remote(
        tokens.at[theirs, :],
        rows_in.at[0, z, :, own_columns],
        tx_s.at[0],
        tx_r.at[0],
        on_p,
    )
    launch(token_copy)
    send_z(0, "across")
    rows_in[0, z, :, own_columns] = tokens[mine, :]
    prepare(1)
    token_copy.wait_recv()
    gather_step(0, 0, 0)
    gather_step(0, 0, 1)
    send_z(0, "beside")
    relay(0, "own")
    prepare(2)
    prepare(3)
    prepare(4)
    prepare(5)
    gather_step(0, 1, 0)
    gather_step(0, 1, 1)
    send_z(0, "beyond")
    relay(0, "across")
    gather_step(0, 2, 0)
    gather_step(0, 2, 1)
    send_z(1, "across", "beyond")
    relay(0, "beside")
    gather_step(0, 3, 0)
    gather_step(0, 3, 1)
    send_z(1, "beside")
    send_z(2, "across", "beyond", "beside")
    relay(0, "beyond")
    relay(1, "own")
    relay(1, "across")
    norm_step(0, 0)
    norm_step(0, 1)
    send_z(3, "across", "beyond", "beside")
    relay(1, "beyond")
    norm_step(0, 2)
    norm_step(0, 3)
    relay(1, "beside")
    relay(2, "own", "across", "beyond", "beside")
    await_weights(0)
    await_weights(1)
    lax.fori_loop(0, 2, lambda i, c: (expand_step(0, i), c)[1], 0)
    await_weights(2)
    lax.fori_loop(0, count, lambda i, c: (contract_step(0, count - 1 - i), c)[1], 0)
    reduce_step(0, 3, 0)
    reduce_step(0, 3, 1)
    relay(3, "own", "across")
    reduce_step(0, 2, 0)
    reduce_step(0, 2, 1)
    relay(3, "beyond")
    reduce_step(0, 1, 0)
    reduce_step(0, 1, 1)
    send_z(4, "across", "beyond")
    relay(3, "beside")
    relay(4, "own")
    reduce_step(0, 0, 0)
    restart(0)
    gather_step(1, 0, 0)
    reduce_step(0, 0, 1)
    restart(1)
    gather_step(1, 0, 1)
    gather_step(1, 1, 0)
    gather_step(1, 1, 1)
    send_z(4, "beside")
    send_z(5, "across")
    gather_step(1, 2, 0)
    gather_step(1, 2, 1)
    send_z(5, "beyond")
    relay(4, "across")
    gather_step(1, 3, 0)
    gather_step(1, 3, 1)
    send_z(5, "beside")
    relay(4, "beyond", "beside")
    relay(5, "own")
    norm_step(1, 0)
    norm_step(1, 1)
    norm_step(1, 2)
    norm_step(1, 3)
    relay(5, "across")
    await_weights(3)
    await_weights(4)
    lax.fori_loop(0, 2, lambda i, c: (expand_step(1, i), c)[1], 0)
    relay(5, "beyond", "beside")
    await_weights(5)
    lax.fori_loop(0, count, lambda i, c: (contract_step(1, count - 1 - i), c)[1], 0)
    reduce_step(1, 3, 0)
    reduce_step(1, 3, 1)
    reduce_step(1, 2, 0)
    reduce_step(1, 2, 1)
    reduce_step(1, 1, 0)
    reduce_step(1, 1, 1)
    reduce_step(1, 0, 0)
    reduce_step(1, 0, 1)
    for h in range(PARTS):
        rows = rows_of(h)
        total[rows] = 0.1 * first[rows] + 0.5 * total[rows] * vectors[3, :, at_half(q)]
    squares = jnp.sum(total[...] * total[...], axis=1, keepdims=True)
    stats[0] = jnp.broadcast_to(squares, (half_rows, 128)).T[:8]
    last[0] = total[:, at_block(1 - p)].astype(jnp.bfloat16)
    ends = [
        remote(stats.at[0], stats.at[1 + n], end_s.at[n], end_r.at[n], target)
        for n, target in enumerate((on_q, on_p, turned(1 - p, 1 - q)))
    ]
    ends.append(remote(last.at[0], last.at[1], end_s.at[3], end_r.at[3], on_p))
    for copy in ends:
        launch(copy)

    def spread(n):
        return jnp.broadcast_to(stats[n][:1], (128, half_rows)).T[:, :1]

    ends[0].wait_recv()
    factor = lax.rsqrt((squares + spread(1)) * (1.0 / width) + 1e-06)
    gains = vectors[4, :, at_block(2 * q + p)]
    out[mine, :] = (total[:, at_block(p)] * factor * gains).astype(jnp.bfloat16)
    ends[1].wait_recv()
    ends[2].wait_recv()
    factor = lax.rsqrt((spread(2) + spread(3)) * (1.0 / width) + 1e-06)
    ends[3].wait_recv()
    out[theirs, :] = (last[1].astype(jnp.float32) * factor * gains).astype(jnp.bfloat16)
    for b in range(2):
        for i in range(count):
            for h in range(PARTS):
                reduce_q(b, i, h).wait_send()
    for m in range(6):
        drain_weights(m)
    for condition, copy in sends:
        if condition is None:
            copy.wait_send()
        else:

            @pl.when(condition)
            def _(copy=copy):
                copy.wait_send()


def fused(tokens, *rest):
    (
        gain_first,
        gate_first,
        gate_first_scale,
        up_first,
        up_first_scale,
        down_first,
        down_first_scale,
        gain_second,
        gate_second,
        gate_second_scale,
        up_second,
        up_second_scale,
        down_second,
        down_second_scale,
        gain_last,
    ) = rest
    chips = lax.axis_size("cb") // 2
    rows, columns = tokens.shape
    piece, units = gate_first.shape
    share = units // chips
    width, half_rows = 4 * columns, rows // 2
    half = width // 2

    def row(vector):
        return vector.reshape(1, -1)

    vmem = pl.BlockSpec(memory_space=pltpu.VMEM)
    anywhere = pl.BlockSpec(memory_space=pl.ANY)
    bf16, f32 = jnp.bfloat16, jnp.float32
    dma = pltpu.SemaphoreType.DMA
    stage_shapes = [w.shape for w in (gate_first, up_first, down_first)] * 2
    moved = pltpu.VMEM((2, chips, half_rows, half), bf16)
    scratch = [pltpu.VMEM(shape, f32) for shape in stage_shapes] + [
        pltpu.VMEM((6, units, piece), bf16),
        pltpu.VMEM((6, 2 * share, width), bf16),
        pltpu.VMEM((2, chips, half_rows, width), bf16),
        pltpu.VMEM((chips * half_rows, width), bf16),
        pltpu.VMEM((chips * half_rows, 2 * share), bf16),
        pltpu.VMEM((chips, half_rows, width), f32),
        moved,
        moved,
        moved,
        moved,
        moved,
        pltpu.VMEM((half_rows, half), f32),
        pltpu.VMEM((half_rows, half), f32),
        pltpu.VMEM((4, 8, half_rows), f32),
        pltpu.VMEM((2, half_rows, columns), bf16),
        pltpu.VMEM((5, 1, width), f32),
        dma((6,)),
        dma((6, chips - 1)),
        dma((6, chips - 1)),
        dma((6, 2)),
        dma((6,)),
        dma((6,)),
        dma((6,)),
        dma((1,)),
        dma((1,)),
        dma((2, PARTS, chips + 1)),
        dma((2, PARTS, chips)),
        dma((2, PARTS, chips)),
        dma((2, PARTS, chips)),
        dma((2, PARTS, chips)),
        dma((2, PARTS, chips)),
        dma((2, PARTS, chips)),
        dma((2, PARTS, chips)),
        dma((2, PARTS, chips)),
        dma((4,)),
        dma((4,)),
    ]
    return pl.pallas_call(
        functools.partial(kernel, chips),
        out_shape=jax.ShapeDtypeStruct(tokens.shape, bf16),
        in_specs=[vmem] * 10 + [anywhere] * 6,
        out_specs=vmem,
        scratch_shapes=scratch,
        compiler_params=pltpu.CompilerParams(
            collective_id=0, has_side_effects=True, vmem_limit_bytes=62 * 2**20
        ),
    )(
        tokens,
        row(gain_first),
        row(down_first_scale),
        row(gain_second),
        row(down_second_scale),
        row(gain_last),
        gate_first_scale,
        up_first_scale,
        gate_second_scale,
        up_second_scale,
        gate_first,
        up_first,
        down_first,
        gate_second,
        up_second,
        down_second,
    )


def plan_for(mesh):
    ra, cb = mesh.shape["ra"], mesh.shape["cb"]

    def run(tokens, *rest):
        units = rest[1].shape[1]
        aligned = units % (cb * 8) == 0 and units % 128 == 0 and tokens.shape[0] % (32 * PARTS) == 0
        if ra == 4 and cb == 8 and aligned:
            return fused(tokens, *rest)
        return shards(tokens, *rest)

    return run


def solution(mesh):
    placed = (
        P("cb", "ra"),
        P(),
        P("cb", "ra"),
        P("ra"),
        P("cb", "ra"),
        P("ra"),
        P("ra", "cb"),
        P(),
        P(),
        P("cb", "ra"),
        P("ra"),
        P("cb", "ra"),
        P("ra"),
        P("ra", "cb"),
        P(),
        P(),
    )
    return jax.shard_map(
        plan_for(mesh), mesh=mesh, in_specs=placed, out_specs=P("cb", "ra"), check_vma=False
    )
```

```python
import functools

import jax
import jax.numpy as jnp
from jax import lax
from jax.experimental import pallas as pl
from jax.experimental.pallas import tpu as pltpu
from jax.sharding import PartitionSpec as P

MESH = pl.DeviceIdType.MESH
PARTS = 2
D = 2048


def own_slice(vector, width):
    return lax.dynamic_slice_in_dim(vector, lax.axis_index("ra") * width, width, 0)


def full_norm(values, gain):
    meansq = jnp.mean(values * values, axis=1, keepdims=True)
    return (values * lax.rsqrt(meansq + 1e-06) * gain).astype(jnp.bfloat16)


def expand(normed, w_gate, s_gate, w_up, s_up, w_down):
    gate = jnp.dot(
        normed,
        lax.all_gather(w_gate.astype(jnp.bfloat16), "cb", axis=0, tiled=True),
        preferred_element_type=jnp.float32,
    )
    upper = jnp.dot(
        normed,
        lax.all_gather(w_up.astype(jnp.bfloat16), "cb", axis=0, tiled=True),
        preferred_element_type=jnp.float32,
    )
    hidden = (jax.nn.silu(gate * s_gate) * (upper * s_up)).astype(jnp.bfloat16)
    return jnp.dot(
        hidden,
        lax.all_gather(w_down.astype(jnp.bfloat16), "cb", axis=1, tiled=True),
        preferred_element_type=jnp.float32,
    )


def reduce_share(partial_value):
    return lax.psum_scatter(
        partial_value.astype(jnp.bfloat16), "ra", scatter_dimension=1, tiled=True
    ).astype(jnp.float32)


def shards(
    tokens,
    gain_first,
    gate_first,
    gate_first_scale,
    up_first,
    up_first_scale,
    down_first,
    down_first_scale,
    gain_second,
    gate_second,
    gate_second_scale,
    up_second,
    up_second_scale,
    down_second,
    down_second_scale,
    gain_last,
):
    width = tokens.shape[1]
    whole_in = lax.all_gather(tokens, "ra", axis=1, tiled=True).astype(jnp.float32)
    normed = full_norm(whole_in, gain_first)
    partial_value = expand(
        normed, gate_first, gate_first_scale, up_first, up_first_scale, down_first
    )
    summed = lax.psum(partial_value.astype(jnp.bfloat16), "ra").astype(jnp.float32)
    first = 0.1 * whole_in + 0.5 * summed * down_first_scale
    first_share = own_slice(first.T, width).T
    normed_next = full_norm(first, gain_second)
    partial_next = expand(
        normed_next, gate_second, gate_second_scale, up_second, up_second_scale, down_second
    )
    second = 0.1 * first_share + 0.5 * reduce_share(partial_next) * own_slice(
        down_second_scale, width
    )
    closing = lax.psum(jnp.sum(second * second, axis=1), "ra")
    return (second * lax.rsqrt(closing / D + 1e-06)[:, None] * own_slice(gain_last, width)).astype(
        jnp.bfloat16
    )


def remote(source, target, sent, received, device):
    return pltpu.make_async_remote_copy(
        src_ref=source,
        dst_ref=target,
        send_sem=sent,
        recv_sem=received,
        device_id=device,
        device_id_type=MESH,
    )


def kernel(chips, *refs):
    (tokens, gain_first, scale_first, gain_second, scale_second, gain_last) = refs[:6]
    scales = refs[6:10]
    weights = refs[10:16]
    out = refs[16]
    stages = refs[17:23]
    (
        sendable,
        whole,
        rows_in,
        normed,
        hidden,
        product,
        given,
        taken,
        passed,
        from_below,
        from_above,
        total,
        first,
        stats,
        last,
        vectors,
        load_sem,
        wz_s,
        wz_r,
        wp_s,
        wp_r,
        wk_s,
        wk_r,
        tx_s,
        tx_r,
        az_s,
        az_r,
        ay_s,
        ay_r,
        ry_s,
        ry_r,
        rz_s,
        rzu_r,
        rzd_r,
        end_s,
        end_r,
    ) = refs[23:]
    count = chips
    half_rows = tokens.shape[0] // 2
    columns = tokens.shape[1]
    width = 4 * columns
    half = width // 2
    units = sendable.shape[1]
    share = units // count
    part_rows = half_rows // PARTS
    piece = sendable.shape[2]

    ra, cb = lax.axis_index("ra"), lax.axis_index("cb")
    y, x = lax.div(ra, 2), lax.rem(ra, 2)
    z, k = lax.div(cb, 2), lax.rem(cb, 2)
    p, q = x + k * (y - x), y + k * (x - y)
    far = lax.div(z, 2)

    def device(x_at, y_at, z_at, k_at):
        return (y_at * 2 + x_at, z_at * 2 + k_at)

    def turned(p_at, q_at):
        return device(p_at + k * (q_at - p_at), q_at + k * (p_at - q_at), z, k)

    on_p, on_q = turned(1 - p, q), turned(p, 1 - q)
    on_k = device(x, y, z, 1 - k)
    to_x, to_y = device(1 - x, y, z, 0), device(x, 1 - y, z, 1)
    above = device(x, y, lax.rem(z + 1, count), k)
    below = device(x, y, lax.rem(z + count - 1, count), k)

    def around(d):
        return lax.rem(z + d, count)

    def near(i):
        outer, inner = i // 2, i % 2
        close = z + inner * (1 - 2 * lax.rem(z, 2))
        distant = (2 + inner) - far * (1 + 2 * inner)
        return (1 - outer) * close + outer * distant

    def natural(block):
        return block if block in (0, 3) else (1 + k if block == 1 else 2 - k)

    def at_share(n):
        return pl.ds(pl.multiple_of(n * share, 16), share)

    def at_column(z_at, k_at):
        return pl.ds(pl.multiple_of(k_at * half + z_at * piece, 128), piece)

    def at_half(h):
        return pl.ds(pl.multiple_of(h * half, 128), half)

    def at_block(n):
        return pl.ds(pl.multiple_of(n * columns, 128), columns)

    sends = []

    def launch(copy):
        copy.start()
        sends.append((None, copy))

    def launch_if(condition, copy):
        @pl.when(condition)
        def _():
            copy.start()

        sends.append((condition, copy))

    barrier = pltpu.get_barrier_semaphore()
    partners = [device(1 - x, y, z, 0), device(1 - x, y, z, 1), device(x, 1 - y, z, 0)]
    partners += [device(x, 1 - y, z, 1), device(1 - x, 1 - y, z, k), on_k]
    partners += [device(x, y, around(d), k) for d in range(1, count)]
    for partner in partners:
        pl.semaphore_signal(barrier, inc=1, device_id=partner, device_id_type=MESH)
    loads = [
        pltpu.make_async_copy(weights[m], stages[m], load_sem.at[m]) for m in range(6)
    ]
    for load in loads:
        load.start()
    for n, vector in enumerate((gain_first, scale_first, gain_second, scale_second, gain_last)):
        for block in range(4):
            vectors[n, :, block * columns : (block + 1) * columns] = vector[
                :, at_block(natural(block))
            ]

    def prepare(m):
        loads[m].wait()
        if m % 3 == 2:
            sendable[m] = stages[m][...].astype(jnp.bfloat16)
        else:
            scale = scales[2 * (m // 3) + m % 3]
            for at in range(0, units, 128):
                block = stages[m][:, at : at + 128] * scale[at : at + 128][None, :]
                sendable[m, at : at + 128, :] = block.T.astype(jnp.bfloat16)
        whole[m, at_share(p), at_column(z, k)] = sendable[m, at_share(z), :]

    def z_copy(m, d):
        return remote(
            sendable.at[m, at_share(around(d)), :],
            whole.at[m, at_share(p), at_column(z, k)],
            wz_s.at[m, d - 1],
            wz_r.at[m, d - 1],
            device(x, y, around(d), k),
        )

    odd = lax.rem(z, 2)
    outgoing = {"across": 2, "beyond": 3 - 2 * odd, "beside": 1 + 2 * odd}
    incoming = {"own": 0, "across": 2, "beyond": 1 + 2 * odd, "beside": 3 - 2 * odd}

    def send_z(m, *steps):
        for step in steps:
            launch(z_copy(m, outgoing[step]))

    def relay(m, *steps):
        for step in steps:
            d = incoming[step]
            place = at_column(around(count - d), k)
            if step != "own":
                z_copy(m, d).wait_recv()
                source = whole.at[m, at_share(p), place]
            else:
                source = sendable.at[m, at_share(z), :]
            remote(
                source, whole.at[m, at_share(x), place], wp_s.at[m, 0], wp_r.at[m], to_x
            ).start()
            remote(
                source, whole.at[m, at_share(y), place], wp_s.at[m, 1], wp_r.at[m], to_y
            ).start()
            remote(
                source, whole.at[m, at_share(q), place], wk_s.at[m], wk_r.at[m], on_k
            ).start()

    def await_weights(m):
        part = whole.at[m, at_share(1 - p), :]
        remote(part, part, wp_s.at[m, 0], wp_r.at[m], on_p).wait_recv()
        part = whole.at[m, at_share(p), at_half(1 - k)]
        remote(part, part, wk_s.at[m], wk_r.at[m], on_k).wait_recv()

    def drain_weights(m):
        part = whole.at[m, at_share(p), at_half(k)]
        remote(part, part, wp_s.at[m, 0], wp_r.at[m], to_x).wait_send()
        remote(part, part, wp_s.at[m, 1], wp_r.at[m], to_y).wait_send()
        remote(part, part, wk_s.at[m], wk_r.at[m], on_k).wait_send()

    def rows_of(h):
        return slice(h * part_rows, (h + 1) * part_rows)

    def gather_z(b, i, h, up):
        j = near(i)
        part = rows_in.at[b, j, rows_of(h), at_half(q)]
        return remote(
            part,
            part,
            az_s.at[b, h, i + (0 if up or i else count)],
            az_r.at[b, h, j],
            above if up else below,
        )

    def gather_q(b, i, h):
        part = rows_in.at[b, near(i), rows_of(h), at_half(q)]
        return remote(part, part, ay_s.at[b, h, i], ay_r.at[b, h, i], on_q)

    def gather_step(b, i, h):
        j = near(i)
        if i == 0:
            launch_if(z < count - 1, gather_z(b, 0, h, True))
            launch_if(z > 0, gather_z(b, 0, h, False))
        else:
            gather_z(b, i, h, True).wait_recv()
            launch_if((j < z) & (z < count - 1), gather_z(b, i, h, True))
            launch_if((j > z) & (z > 0), gather_z(b, i, h, False))
        launch(gather_q(b, i, h))

    def norm_step(b, i):
        j = near(i)
        for h in range(PARTS):
            gather_q(b, i, h).wait_recv()
        values = rows_in[b, j].astype(jnp.float32)
        meansq = jnp.sum(values * values, axis=1, keepdims=True) * (1.0 / width)
        values = values * lax.rsqrt(meansq + 1e-06) * vectors[2 * b]
        values = values.astype(jnp.bfloat16)
        rows = slice(i * half_rows, (i + 1) * half_rows)
        for block in range(4):
            for side in range(2):
                at = block * columns + side * piece
                normed[rows, at_column(natural(block), side)] = values[:, at : at + piece]

    def expand_step(b, pair):
        axes = (((1,), (1,)), ((), ()))
        rows = pl.ds(pl.multiple_of(pair * 2 * half_rows, 16), 2 * half_rows)
        gate = lax.dot_general(
            normed[rows, :], whole[3 * b], axes, preferred_element_type=jnp.float32
        )
        upper = lax.dot_general(
            normed[rows, :], whole[3 * b + 1], axes, preferred_element_type=jnp.float32
        )
        hidden[rows, :] = (gate / (1.0 + jnp.exp(-gate)) * upper).astype(jnp.bfloat16)

    def reduce_q(b, i, h):
        j = near(i)
        return remote(
            given.at[b, j, rows_of(h)],
            taken.at[b, j, rows_of(h)],
            ry_s.at[b, h, i],
            ry_r.at[b, h, i],
            on_q,
        )

    def contract_step(b, i):
        j = near(i)
        rows = pl.ds(pl.multiple_of(i * half_rows, 16), half_rows)
        for side in range(2):
            part = jnp.dot(
                hidden[rows, :],
                whole[3 * b + 2, :, side * half : (side + 1) * half],
                preferred_element_type=jnp.float32,
            )
            for block in range(4):
                at = pl.multiple_of(natural(block) * columns + side * piece, 128)
                product[j, :, pl.ds(at, piece)] = part[:, block * piece : (block + 1) * piece]
        given[b, j] = product[j, :, at_half(1 - q)].astype(jnp.bfloat16)
        for h in range(PARTS):
            reduce_q(b, i, h).start()

    def reduce_z(b, i, h, up):
        j = near(i)
        landing, arrived, target = (
            (from_below, rzu_r, above) if up else (from_above, rzd_r, below)
        )
        return remote(
            passed.at[b, j, rows_of(h)],
            landing.at[b, j, rows_of(h)],
            rz_s.at[b, h, i],
            arrived.at[b, h, j],
            target,
        )

    def reduce_step(b, i, h):
        j = near(i)
        rows = rows_of(h)
        reduce_q(b, i, h).wait_recv()
        total[rows] = product[j, rows, at_half(q)] + taken[b, j, rows].astype(jnp.float32)
        rises = (j >= z) & (z > 0)
        falls = (j <= z) & (z < count - 1)

        @pl.when(rises)
        def _():
            reduce_z(b, i, h, True).wait_recv()
            total[rows] += from_below[b, j, rows].astype(jnp.float32)

        @pl.when(falls)
        def _():
            reduce_z(b, i, h, False).wait_recv()
            total[rows] += from_above[b, j, rows].astype(jnp.float32)

        if i:
            passed[b, j, rows] = total[rows].astype(jnp.bfloat16)
            launch_if(j > z, reduce_z(b, i, h, True))
            launch_if(j < z, reduce_z(b, i, h, False))

    def restart(h):
        rows = rows_of(h)
        start = rows_in[0, z, rows, at_half(q)].astype(jnp.float32)
        first[rows] = 0.1 * start + 0.5 * total[rows] * vectors[1, :, at_half(q)]
        rows_in[1, z, rows, at_half(q)] = first[rows].astype(jnp.bfloat16)

    gains = vectors[4, :, at_block(2 * q + p)]

    def end_copies(h):
        copies = [
            remote(stats.at[0, h], stats.at[1 + n, h], end_s.at[h, n], end_r.at[h, n], target)
            for n, target in enumerate((on_q, on_p, turned(1 - p, 1 - q)))
        ]
        part = rows_of(h)
        copies.append(
            remote(last.at[0, part], last.at[1, part], end_s.at[h, 3], end_r.at[h, 3], on_p)
        )
        return copies

    def spread(n, h):
        return jnp.broadcast_to(stats[n, h][:1], (128, part_rows)).T[:, :1]

    def end_step(h):
        rows = rows_of(h)
        total[rows] = 0.1 * first[rows] + 0.5 * total[rows] * vectors[3, :, at_half(q)]
        squares = jnp.sum(total[rows] * total[rows], axis=1, keepdims=True)
        stats[0, h] = jnp.broadcast_to(squares, (part_rows, 128)).T[:8]
        last[0, rows] = total[rows, at_block(1 - p)].astype(jnp.bfloat16)
        for copy in end_copies(h):
            launch(copy)

    def finish_step(h):
        rows = rows_of(h)
        copies = end_copies(h)
        copies[0].wait_recv()
        factor = lax.rsqrt((spread(0, h) + spread(1, h)) * (1.0 / width) + 1e-06)
        own = pl.ds(pl.multiple_of(p * half_rows + h * part_rows, 16), part_rows)
        out[own, :] = (total[rows, at_block(p)] * factor * gains).astype(jnp.bfloat16)
        for copy in copies[1:]:
            copy.wait_recv()
        factor = lax.rsqrt((spread(2, h) + spread(3, h)) * (1.0 / width) + 1e-06)
        other = pl.ds(pl.multiple_of((1 - p) * half_rows + h * part_rows, 16), part_rows)
        out[other, :] = (last[1, rows].astype(jnp.float32) * factor * gains).astype(jnp.bfloat16)

    prepare(0)
    pl.semaphore_wait(barrier, len(partners))

    mine = pl.ds(pl.multiple_of(p * half_rows, 16), half_rows)
    theirs = pl.ds(pl.multiple_of((1 - p) * half_rows, 16), half_rows)
    own_columns = at_block(2 * q + p)
    token_copy = remote(
        tokens.at[theirs, :],
        rows_in.at[0, z, :, own_columns],
        tx_s.at[0],
        tx_r.at[0],
        on_p,
    )
    launch(token_copy)
    send_z(0, "across")
    rows_in[0, z, :, own_columns] = tokens[mine, :]
    prepare(1)
    token_copy.wait_recv()
    gather_step(0, 0, 0)
    gather_step(0, 0, 1)
    send_z(0, "beside")
    relay(0, "own")
    prepare(2)
    prepare(3)
    prepare(4)
    prepare(5)
    gather_step(0, 1, 0)
    gather_step(0, 1, 1)
    send_z(0, "beyond")
    send_z(1, "across", "beyond")
    relay(0, "across")
    relay(1, "own")
    gather_step(0, 2, 0)
    gather_step(0, 2, 1)
    send_z(1, "beside")
    send_z(2, "across")
    relay(0, "beside")
    gather_step(0, 3, 0)
    gather_step(0, 3, 1)
    send_z(2, "beyond", "beside")
    relay(0, "beyond")
    relay(1, "across")
    norm_step(0, 0)
    norm_step(0, 1)
    send_z(3, "across", "beyond", "beside")
    relay(1, "beyond")
    norm_step(0, 2)
    norm_step(0, 3)
    relay(1, "beside")
    relay(2, "own", "across", "beyond", "beside")
    send_z(4, "across", "beyond", "beside")
    await_weights(0)
    await_weights(1)
    lax.fori_loop(0, 2, lambda i, c: (expand_step(0, i), c)[1], 0)
    await_weights(2)
    lax.fori_loop(0, count, lambda i, c: (contract_step(0, count - 1 - i), c)[1], 0)
    reduce_step(0, 3, 0)
    reduce_step(0, 3, 1)
    relay(3, "own", "across")
    reduce_step(0, 2, 0)
    reduce_step(0, 2, 1)
    relay(3, "beyond")
    reduce_step(0, 1, 0)
    reduce_step(0, 1, 1)
    relay(3, "beside")
    relay(4, "own")
    reduce_step(0, 0, 0)
    restart(0)
    gather_step(1, 0, 0)
    reduce_step(0, 0, 1)
    restart(1)
    gather_step(1, 0, 1)
    relay(4, "across")
    gather_step(1, 1, 0)
    gather_step(1, 1, 1)
    relay(4, "beyond")
    send_z(5, "across")
    gather_step(1, 2, 0)
    gather_step(1, 2, 1)
    relay(4, "beside")
    send_z(5, "beyond")
    gather_step(1, 3, 0)
    gather_step(1, 3, 1)
    send_z(5, "beside")
    relay(5, "own")
    norm_step(1, 0)
    norm_step(1, 1)
    norm_step(1, 2)
    norm_step(1, 3)
    await_weights(3)
    await_weights(4)
    relay(5, "across")
    lax.fori_loop(0, 2, lambda i, c: (expand_step(1, i), c)[1], 0)
    relay(5, "beyond", "beside")
    await_weights(5)
    lax.fori_loop(0, count, lambda i, c: (contract_step(1, count - 1 - i), c)[1], 0)
    reduce_step(1, 3, 0)
    reduce_step(1, 3, 1)
    reduce_step(1, 2, 0)
    reduce_step(1, 2, 1)
    reduce_step(1, 1, 0)
    reduce_step(1, 1, 1)
    reduce_step(1, 0, 0)
    end_step(0)
    reduce_step(1, 0, 1)
    end_step(1)
    finish_step(0)
    finish_step(1)
    for b in range(2):
        for i in range(count):
            for h in range(PARTS):
                reduce_q(b, i, h).wait_send()
    for m in range(6):
        drain_weights(m)
    for condition, copy in sends:
        if condition is None:
            copy.wait_send()
        else:

            @pl.when(condition)
            def _(copy=copy):
                copy.wait_send()


def fused(tokens, *rest):
    (
        gain_first,
        gate_first,
        gate_first_scale,
        up_first,
        up_first_scale,
        down_first,
        down_first_scale,
        gain_second,
        gate_second,
        gate_second_scale,
        up_second,
        up_second_scale,
        down_second,
        down_second_scale,
        gain_last,
    ) = rest
    chips = lax.axis_size("cb") // 2
    rows, columns = tokens.shape
    piece, units = gate_first.shape
    share = units // chips
    width, half_rows = 4 * columns, rows // 2
    half = width // 2

    def row(vector):
        return vector.reshape(1, -1)

    vmem = pl.BlockSpec(memory_space=pltpu.VMEM)
    anywhere = pl.BlockSpec(memory_space=pl.ANY)
    bf16, f32 = jnp.bfloat16, jnp.float32
    dma = pltpu.SemaphoreType.DMA
    stage_shapes = [w.shape for w in (gate_first, up_first, down_first)] * 2
    moved = pltpu.VMEM((2, chips, half_rows, half), bf16)
    scratch = [pltpu.VMEM(shape, f32) for shape in stage_shapes] + [
        pltpu.VMEM((6, units, piece), bf16),
        pltpu.VMEM((6, 2 * share, width), bf16),
        pltpu.VMEM((2, chips, half_rows, width), bf16),
        pltpu.VMEM((chips * half_rows, width), bf16),
        pltpu.VMEM((chips * half_rows, 2 * share), bf16),
        pltpu.VMEM((chips, half_rows, width), f32),
        moved,
        moved,
        moved,
        moved,
        moved,
        pltpu.VMEM((half_rows, half), f32),
        pltpu.VMEM((half_rows, half), f32),
        pltpu.VMEM((4, PARTS, 8, half_rows // PARTS), f32),
        pltpu.VMEM((2, half_rows, columns), bf16),
        pltpu.VMEM((5, 1, width), f32),
        dma((6,)),
        dma((6, chips - 1)),
        dma((6, chips - 1)),
        dma((6, 2)),
        dma((6,)),
        dma((6,)),
        dma((6,)),
        dma((1,)),
        dma((1,)),
        dma((2, PARTS, chips + 1)),
        dma((2, PARTS, chips)),
        dma((2, PARTS, chips)),
        dma((2, PARTS, chips)),
        dma((2, PARTS, chips)),
        dma((2, PARTS, chips)),
        dma((2, PARTS, chips)),
        dma((2, PARTS, chips)),
        dma((2, PARTS, chips)),
        dma((PARTS, 4)),
        dma((PARTS, 4)),
    ]
    return pl.pallas_call(
        functools.partial(kernel, chips),
        out_shape=jax.ShapeDtypeStruct(tokens.shape, bf16),
        in_specs=[vmem] * 10 + [anywhere] * 6,
        out_specs=vmem,
        scratch_shapes=scratch,
        compiler_params=pltpu.CompilerParams(
            collective_id=0, has_side_effects=True, vmem_limit_bytes=62 * 2**20
        ),
    )(
        tokens,
        row(gain_first),
        row(down_first_scale),
        row(gain_second),
        row(down_second_scale),
        row(gain_last),
        gate_first_scale,
        up_first_scale,
        gate_second_scale,
        up_second_scale,
        gate_first,
        up_first,
        down_first,
        gate_second,
        up_second,
        down_second,
    )


def plan_for(mesh):
    ra, cb = mesh.shape["ra"], mesh.shape["cb"]

    def run(tokens, *rest):
        units = rest[1].shape[1]
        aligned = units % (cb * 8) == 0 and units % 128 == 0 and tokens.shape[0] % (32 * PARTS) == 0
        if ra == 4 and cb == 8 and aligned:
            return fused(tokens, *rest)
        return shards(tokens, *rest)

    return run


def solution(mesh):
    placed = (
        P("cb", "ra"),
        P(),
        P("cb", "ra"),
        P("ra"),
        P("cb", "ra"),
        P("ra"),
        P("ra", "cb"),
        P(),
        P(),
        P("cb", "ra"),
        P("ra"),
        P("cb", "ra"),
        P("ra"),
        P("ra", "cb"),
        P(),
        P(),
    )
    return jax.shard_map(
        plan_for(mesh), mesh=mesh, in_specs=placed, out_specs=P("cb", "ra"), check_vma=False
    )
```

```python
import functools

import jax
import jax.numpy as jnp
from jax import lax
from jax.experimental import pallas as pl
from jax.experimental.pallas import tpu as pltpu
from jax.sharding import PartitionSpec as P

MESH = pl.DeviceIdType.MESH
PARTS = 2
D = 2048


def own_slice(vector, width):
    return lax.dynamic_slice_in_dim(vector, lax.axis_index("ra") * width, width, 0)


def full_norm(values, gain):
    meansq = jnp.mean(values * values, axis=1, keepdims=True)
    return (values * lax.rsqrt(meansq + 1e-06) * gain).astype(jnp.bfloat16)


def expand(normed, w_gate, s_gate, w_up, s_up, w_down):
    gate = jnp.dot(
        normed,
        lax.all_gather(w_gate.astype(jnp.bfloat16), "cb", axis=0, tiled=True),
        preferred_element_type=jnp.float32,
    )
    upper = jnp.dot(
        normed,
        lax.all_gather(w_up.astype(jnp.bfloat16), "cb", axis=0, tiled=True),
        preferred_element_type=jnp.float32,
    )
    hidden = (jax.nn.silu(gate * s_gate) * (upper * s_up)).astype(jnp.bfloat16)
    return jnp.dot(
        hidden,
        lax.all_gather(w_down.astype(jnp.bfloat16), "cb", axis=1, tiled=True),
        preferred_element_type=jnp.float32,
    )


def reduce_share(partial_value):
    return lax.psum_scatter(
        partial_value.astype(jnp.bfloat16), "ra", scatter_dimension=1, tiled=True
    ).astype(jnp.float32)


def shards(
    tokens,
    gain_first,
    gate_first,
    gate_first_scale,
    up_first,
    up_first_scale,
    down_first,
    down_first_scale,
    gain_second,
    gate_second,
    gate_second_scale,
    up_second,
    up_second_scale,
    down_second,
    down_second_scale,
    gain_last,
):
    width = tokens.shape[1]
    whole_in = lax.all_gather(tokens, "ra", axis=1, tiled=True).astype(jnp.float32)
    normed = full_norm(whole_in, gain_first)
    partial_value = expand(
        normed, gate_first, gate_first_scale, up_first, up_first_scale, down_first
    )
    summed = lax.psum(partial_value.astype(jnp.bfloat16), "ra").astype(jnp.float32)
    first = 0.1 * whole_in + 0.5 * summed * down_first_scale
    first_share = own_slice(first.T, width).T
    normed_next = full_norm(first, gain_second)
    partial_next = expand(
        normed_next, gate_second, gate_second_scale, up_second, up_second_scale, down_second
    )
    second = 0.1 * first_share + 0.5 * reduce_share(partial_next) * own_slice(
        down_second_scale, width
    )
    closing = lax.psum(jnp.sum(second * second, axis=1), "ra")
    return (second * lax.rsqrt(closing / D + 1e-06)[:, None] * own_slice(gain_last, width)).astype(
        jnp.bfloat16
    )


def remote(source, target, sent, received, device):
    return pltpu.make_async_remote_copy(
        src_ref=source,
        dst_ref=target,
        send_sem=sent,
        recv_sem=received,
        device_id=device,
        device_id_type=MESH,
    )


def kernel(chips, *refs):
    (tokens, gain_first, scale_first, gain_second, scale_second, gain_last) = refs[:6]
    scales = refs[6:10]
    weights = refs[10:16]
    out = refs[16]
    stages = refs[17:23]
    (
        sendable,
        whole,
        rows_in,
        normed,
        hidden,
        product,
        given,
        taken,
        passed,
        from_below,
        from_above,
        total,
        first,
        stats,
        last,
        vectors,
        load_sem,
        wz_s,
        wz_r,
        wp_s,
        wp_r,
        wk_s,
        wk_r,
        tx_s,
        tx_r,
        az_s,
        az_r,
        ay_s,
        ay_r,
        ry_s,
        ry_r,
        rz_s,
        rzu_r,
        rzd_r,
        end_s,
        end_r,
    ) = refs[23:]
    count = chips
    half_rows = tokens.shape[0] // 2
    columns = tokens.shape[1]
    width = 4 * columns
    half = width // 2
    units = sendable.shape[1]
    share = units // count
    part_rows = half_rows // PARTS
    piece = sendable.shape[2]

    ra, cb = lax.axis_index("ra"), lax.axis_index("cb")
    y, x = lax.div(ra, 2), lax.rem(ra, 2)
    z, k = lax.div(cb, 2), lax.rem(cb, 2)
    p, q = x + k * (y - x), y + k * (x - y)
    far = lax.div(z, 2)

    def device(x_at, y_at, z_at, k_at):
        return (y_at * 2 + x_at, z_at * 2 + k_at)

    def turned(p_at, q_at):
        return device(p_at + k * (q_at - p_at), q_at + k * (p_at - q_at), z, k)

    on_p, on_q = turned(1 - p, q), turned(p, 1 - q)
    on_k = device(x, y, z, 1 - k)
    to_x, to_y = device(1 - x, y, z, 0), device(x, 1 - y, z, 1)
    above = device(x, y, lax.rem(z + 1, count), k)
    below = device(x, y, lax.rem(z + count - 1, count), k)

    def around(d):
        return lax.rem(z + d, count)

    def near(i):
        outer, inner = i // 2, i % 2
        close = z + inner * (1 - 2 * lax.rem(z, 2))
        distant = (2 + inner) - far * (1 + 2 * inner)
        return (1 - outer) * close + outer * distant

    def natural(block):
        return block if block in (0, 3) else (1 + k if block == 1 else 2 - k)

    def at_share(n):
        return pl.ds(pl.multiple_of(n * share, 16), share)

    def at_column(z_at, k_at):
        return pl.ds(pl.multiple_of(k_at * half + z_at * piece, 128), piece)

    def at_half(h):
        return pl.ds(pl.multiple_of(h * half, 128), half)

    def at_block(n):
        return pl.ds(pl.multiple_of(n * columns, 128), columns)

    sends = []

    def launch(copy):
        copy.start()
        sends.append((None, copy))

    def launch_if(condition, copy):
        @pl.when(condition)
        def _():
            copy.start()

        sends.append((condition, copy))

    barrier = pltpu.get_barrier_semaphore()
    partners = [device(1 - x, y, z, 0), device(1 - x, y, z, 1), device(x, 1 - y, z, 0)]
    partners += [device(x, 1 - y, z, 1), device(1 - x, 1 - y, z, k), on_k]
    partners += [device(x, y, around(d), k) for d in range(1, count)]
    for partner in partners:
        pl.semaphore_signal(barrier, inc=1, device_id=partner, device_id_type=MESH)
    loads = [
        pltpu.make_async_copy(weights[m], stages[m], load_sem.at[m]) for m in range(6)
    ]
    for load in loads:
        load.start()
    for n, vector in enumerate((gain_first, scale_first, gain_second, scale_second, gain_last)):
        for block in range(4):
            vectors[n, :, block * columns : (block + 1) * columns] = vector[
                :, at_block(natural(block))
            ]

    def prepare(m):
        loads[m].wait()
        if m % 3 == 2:
            sendable[m] = stages[m][...].astype(jnp.bfloat16)
        else:
            scale = scales[2 * (m // 3) + m % 3]
            for at in range(0, units, 128):
                block = stages[m][:, at : at + 128] * scale[at : at + 128][None, :]
                sendable[m, at : at + 128, :] = block.T.astype(jnp.bfloat16)
        whole[m, at_share(p), at_column(z, k)] = sendable[m, at_share(z), :]

    def z_copy(m, d):
        return remote(
            sendable.at[m, at_share(around(d)), :],
            whole.at[m, at_share(p), at_column(z, k)],
            wz_s.at[m, d - 1],
            wz_r.at[m, d - 1],
            device(x, y, around(d), k),
        )

    odd = lax.rem(z, 2)
    outgoing = {"across": 2, "beyond": 3 - 2 * odd, "beside": 1 + 2 * odd}
    incoming = {"own": 0, "across": 2, "beyond": 1 + 2 * odd, "beside": 3 - 2 * odd}

    def send_z(m, *steps):
        for step in steps:
            launch(z_copy(m, outgoing[step]))

    def relay(m, *steps):
        for step in steps:
            d = incoming[step]
            place = at_column(around(count - d), k)
            if step != "own":
                z_copy(m, d).wait_recv()
                source = whole.at[m, at_share(p), place]
            else:
                source = sendable.at[m, at_share(z), :]
            remote(
                source, whole.at[m, at_share(x), place], wp_s.at[m, 0], wp_r.at[m], to_x
            ).start()
            remote(
                source, whole.at[m, at_share(y), place], wp_s.at[m, 1], wp_r.at[m], to_y
            ).start()
            remote(
                source, whole.at[m, at_share(q), place], wk_s.at[m], wk_r.at[m], on_k
            ).start()

    def await_weights(m):
        part = whole.at[m, at_share(1 - p), :]
        remote(part, part, wp_s.at[m, 0], wp_r.at[m], on_p).wait_recv()
        part = whole.at[m, at_share(p), at_half(1 - k)]
        remote(part, part, wk_s.at[m], wk_r.at[m], on_k).wait_recv()

    def drain_weights(m):
        part = whole.at[m, at_share(p), at_half(k)]
        remote(part, part, wp_s.at[m, 0], wp_r.at[m], to_x).wait_send()
        remote(part, part, wp_s.at[m, 1], wp_r.at[m], to_y).wait_send()
        remote(part, part, wk_s.at[m], wk_r.at[m], on_k).wait_send()

    def rows_of(h):
        return slice(h * part_rows, (h + 1) * part_rows)

    def gather_z(b, i, h, up):
        j = near(i)
        part = rows_in.at[b, j, rows_of(h), at_half(q)]
        return remote(
            part,
            part,
            az_s.at[b, h, i + (0 if up or i else count)],
            az_r.at[b, h, j],
            above if up else below,
        )

    def gather_q(b, i, h):
        part = rows_in.at[b, near(i), rows_of(h), at_half(q)]
        return remote(part, part, ay_s.at[b, h, i], ay_r.at[b, h, i], on_q)

    def gather_step(b, i, h):
        j = near(i)
        if i == 0:
            launch_if(z < count - 1, gather_z(b, 0, h, True))
            launch_if(z > 0, gather_z(b, 0, h, False))
        else:
            gather_z(b, i, h, True).wait_recv()
            launch_if((j < z) & (z < count - 1), gather_z(b, i, h, True))
            launch_if((j > z) & (z > 0), gather_z(b, i, h, False))
        launch(gather_q(b, i, h))

    def norm_step(b, i):
        j = near(i)
        for h in range(PARTS):
            gather_q(b, i, h).wait_recv()
        values = rows_in[b, j].astype(jnp.float32)
        meansq = jnp.sum(values * values, axis=1, keepdims=True) * (1.0 / width)
        values = values * lax.rsqrt(meansq + 1e-06) * vectors[2 * b]
        values = values.astype(jnp.bfloat16)
        rows = slice(i * half_rows, (i + 1) * half_rows)
        for block in range(4):
            for side in range(2):
                at = block * columns + side * piece
                normed[rows, at_column(natural(block), side)] = values[:, at : at + piece]

    def expand_step(b, pair):
        axes = (((1,), (1,)), ((), ()))
        rows = pl.ds(pl.multiple_of(pair * 2 * half_rows, 16), 2 * half_rows)
        gate = lax.dot_general(
            normed[rows, :], whole[3 * b], axes, preferred_element_type=jnp.float32
        )
        upper = lax.dot_general(
            normed[rows, :], whole[3 * b + 1], axes, preferred_element_type=jnp.float32
        )
        hidden[rows, :] = (gate / (1.0 + jnp.exp(-gate)) * upper).astype(jnp.bfloat16)

    def reduce_q(b, i, h):
        j = near(i)
        return remote(
            given.at[b, j, rows_of(h)],
            taken.at[b, j, rows_of(h)],
            ry_s.at[b, h, i],
            ry_r.at[b, h, i],
            on_q,
        )

    def contract_step(b, i):
        j = near(i)
        rows = pl.ds(pl.multiple_of(i * half_rows, 16), half_rows)
        for side in range(2):
            part = jnp.dot(
                hidden[rows, :],
                whole[3 * b + 2, :, side * half : (side + 1) * half],
                preferred_element_type=jnp.float32,
            )
            for block in range(4):
                at = pl.multiple_of(natural(block) * columns + side * piece, 128)
                product[j, :, pl.ds(at, piece)] = part[:, block * piece : (block + 1) * piece]
        given[b, j] = product[j, :, at_half(1 - q)].astype(jnp.bfloat16)
        for h in range(PARTS):
            reduce_q(b, i, h).start()

    def reduce_z(b, i, h, up):
        j = near(i)
        landing, arrived, target = (
            (from_below, rzu_r, above) if up else (from_above, rzd_r, below)
        )
        return remote(
            passed.at[b, j, rows_of(h)],
            landing.at[b, j, rows_of(h)],
            rz_s.at[b, h, i],
            arrived.at[b, h, j],
            target,
        )

    def reduce_step(b, i, h):
        j = near(i)
        rows = rows_of(h)
        reduce_q(b, i, h).wait_recv()
        total[rows] = product[j, rows, at_half(q)] + taken[b, j, rows].astype(jnp.float32)
        rises = (j >= z) & (z > 0)
        falls = (j <= z) & (z < count - 1)

        @pl.when(rises)
        def _():
            reduce_z(b, i, h, True).wait_recv()
            total[rows] += from_below[b, j, rows].astype(jnp.float32)

        @pl.when(falls)
        def _():
            reduce_z(b, i, h, False).wait_recv()
            total[rows] += from_above[b, j, rows].astype(jnp.float32)

        if i:
            passed[b, j, rows] = total[rows].astype(jnp.bfloat16)
            launch_if(j > z, reduce_z(b, i, h, True))
            launch_if(j < z, reduce_z(b, i, h, False))

    def restart(h):
        rows = rows_of(h)
        start = rows_in[0, z, rows, at_half(q)].astype(jnp.float32)
        first[rows] = 0.1 * start + 0.5 * total[rows] * vectors[1, :, at_half(q)]
        rows_in[1, z, rows, at_half(q)] = first[rows].astype(jnp.bfloat16)

    gains = vectors[4, :, at_block(2 * q + p)]

    def settle(copies):
        for condition, copy in copies:
            if condition is None:
                copy.wait_send()
            else:

                @pl.when(condition)
                def _(copy=copy):
                    copy.wait_send()

    def settle_early(copies):
        settle(copies)
        for m in range(6):
            drain_weights(m)
        for i in range(count):
            for h in range(PARTS):
                reduce_q(0, i, h).wait_send()

    def end_copies(h):
        copies = [
            remote(stats.at[0, h], stats.at[1 + n, h], end_s.at[h, n], end_r.at[h, n], target)
            for n, target in enumerate((on_q, on_p, turned(1 - p, 1 - q)))
        ]
        part = rows_of(h)
        copies.append(
            remote(last.at[0, part], last.at[1, part], end_s.at[h, 3], end_r.at[h, 3], on_p)
        )
        return copies

    def spread(n, h):
        return jnp.broadcast_to(stats[n, h][:1], (128, part_rows)).T[:, :1]

    def end_step(h):
        rows = rows_of(h)
        total[rows] = 0.1 * first[rows] + 0.5 * total[rows] * vectors[3, :, at_half(q)]
        squares = jnp.sum(total[rows] * total[rows], axis=1, keepdims=True)
        stats[0, h] = jnp.broadcast_to(squares, (part_rows, 128)).T[:8]
        last[0, rows] = total[rows, at_block(1 - p)].astype(jnp.bfloat16)
        for copy in end_copies(h):
            launch(copy)

    def finish_step(h):
        rows = rows_of(h)
        copies = end_copies(h)
        copies[0].wait_recv()
        factor = lax.rsqrt((spread(0, h) + spread(1, h)) * (1.0 / width) + 1e-06)
        own = pl.ds(pl.multiple_of(p * half_rows + h * part_rows, 16), part_rows)
        out[own, :] = (total[rows, at_block(p)] * factor * gains).astype(jnp.bfloat16)
        for copy in copies[1:]:
            copy.wait_recv()
        factor = lax.rsqrt((spread(2, h) + spread(3, h)) * (1.0 / width) + 1e-06)
        other = pl.ds(pl.multiple_of((1 - p) * half_rows + h * part_rows, 16), part_rows)
        out[other, :] = (last[1, rows].astype(jnp.float32) * factor * gains).astype(jnp.bfloat16)

    prepare(0)
    pl.semaphore_wait(barrier, len(partners))

    mine = pl.ds(pl.multiple_of(p * half_rows, 16), half_rows)
    theirs = pl.ds(pl.multiple_of((1 - p) * half_rows, 16), half_rows)
    own_columns = at_block(2 * q + p)
    token_copy = remote(
        tokens.at[theirs, :],
        rows_in.at[0, z, :, own_columns],
        tx_s.at[0],
        tx_r.at[0],
        on_p,
    )
    launch(token_copy)
    send_z(0, "across")
    rows_in[0, z, :, own_columns] = tokens[mine, :]
    prepare(1)
    token_copy.wait_recv()
    gather_step(0, 0, 0)
    gather_step(0, 0, 1)
    send_z(0, "beside")
    relay(0, "own")
    prepare(2)
    prepare(3)
    prepare(4)
    prepare(5)
    gather_step(0, 1, 0)
    gather_step(0, 1, 1)
    send_z(0, "beyond")
    send_z(1, "across", "beyond")
    relay(0, "across")
    relay(1, "own")
    gather_step(0, 2, 0)
    gather_step(0, 2, 1)
    send_z(1, "beside")
    send_z(2, "across")
    relay(0, "beside")
    gather_step(0, 3, 0)
    gather_step(0, 3, 1)
    send_z(2, "beyond", "beside")
    relay(0, "beyond")
    relay(1, "across")
    norm_step(0, 0)
    norm_step(0, 1)
    send_z(3, "across", "beyond", "beside")
    relay(1, "beyond")
    norm_step(0, 2)
    norm_step(0, 3)
    relay(1, "beside")
    relay(2, "own", "across", "beyond", "beside")
    send_z(4, "across", "beyond", "beside")
    await_weights(0)
    await_weights(1)
    lax.fori_loop(0, 2, lambda i, c: (expand_step(0, i), c)[1], 0)
    await_weights(2)
    lax.fori_loop(0, count, lambda i, c: (contract_step(0, count - 1 - i), c)[1], 0)
    reduce_step(0, 3, 0)
    reduce_step(0, 3, 1)
    relay(3, "own", "across")
    reduce_step(0, 2, 0)
    reduce_step(0, 2, 1)
    relay(3, "beyond")
    reduce_step(0, 1, 0)
    reduce_step(0, 1, 1)
    relay(3, "beside")
    relay(4, "own")
    reduce_step(0, 0, 0)
    restart(0)
    gather_step(1, 0, 0)
    reduce_step(0, 0, 1)
    restart(1)
    gather_step(1, 0, 1)
    relay(4, "across")
    gather_step(1, 1, 0)
    gather_step(1, 1, 1)
    relay(4, "beyond")
    send_z(5, "across")
    gather_step(1, 2, 0)
    gather_step(1, 2, 1)
    relay(4, "beside")
    send_z(5, "beyond")
    gather_step(1, 3, 0)
    gather_step(1, 3, 1)
    send_z(5, "beside")
    relay(5, "own", "across")
    norm_step(1, 0)
    norm_step(1, 1)
    norm_step(1, 2)
    norm_step(1, 3)
    await_weights(3)
    await_weights(4)
    relay(5, "beyond")
    lax.fori_loop(0, 2, lambda i, c: (expand_step(1, i), c)[1], 0)
    relay(5, "beside")
    await_weights(5)
    settled = len(sends)
    lax.fori_loop(0, count, lambda i, c: (contract_step(1, count - 1 - i), c)[1], 0)
    reduce_step(1, 3, 0)
    reduce_step(1, 3, 1)
    reduce_step(1, 2, 0)
    reduce_step(1, 2, 1)
    reduce_step(1, 1, 0)
    reduce_step(1, 1, 1)
    settle_early(sends[:settled])
    reduce_step(1, 0, 0)
    end_step(0)
    reduce_step(1, 0, 1)
    end_step(1)
    finish_step(0)
    finish_step(1)
    for i in range(count):
        for h in range(PARTS):
            reduce_q(1, i, h).wait_send()
    settle(sends[settled:])


def fused(tokens, *rest):
    (
        gain_first,
        gate_first,
        gate_first_scale,
        up_first,
        up_first_scale,
        down_first,
        down_first_scale,
        gain_second,
        gate_second,
        gate_second_scale,
        up_second,
        up_second_scale,
        down_second,
        down_second_scale,
        gain_last,
    ) = rest
    chips = lax.axis_size("cb") // 2
    rows, columns = tokens.shape
    piece, units = gate_first.shape
    share = units // chips
    width, half_rows = 4 * columns, rows // 2
    half = width // 2

    def row(vector):
        return vector.reshape(1, -1)

    vmem = pl.BlockSpec(memory_space=pltpu.VMEM)
    anywhere = pl.BlockSpec(memory_space=pl.ANY)
    bf16, f32 = jnp.bfloat16, jnp.float32
    dma = pltpu.SemaphoreType.DMA
    stage_shapes = [w.shape for w in (gate_first, up_first, down_first)] * 2
    moved = pltpu.VMEM((2, chips, half_rows, half), bf16)
    scratch = [pltpu.VMEM(shape, f32) for shape in stage_shapes] + [
        pltpu.VMEM((6, units, piece), bf16),
        pltpu.VMEM((6, 2 * share, width), bf16),
        pltpu.VMEM((2, chips, half_rows, width), bf16),
        pltpu.VMEM((chips * half_rows, width), bf16),
        pltpu.VMEM((chips * half_rows, 2 * share), bf16),
        pltpu.VMEM((chips, half_rows, width), f32),
        moved,
        moved,
        moved,
        moved,
        moved,
        pltpu.VMEM((half_rows, half), f32),
        pltpu.VMEM((half_rows, half), f32),
        pltpu.VMEM((4, PARTS, 8, half_rows // PARTS), f32),
        pltpu.VMEM((2, half_rows, columns), bf16),
        pltpu.VMEM((5, 1, width), f32),
        dma((6,)),
        dma((6, chips - 1)),
        dma((6, chips - 1)),
        dma((6, 2)),
        dma((6,)),
        dma((6,)),
        dma((6,)),
        dma((1,)),
        dma((1,)),
        dma((2, PARTS, chips + 1)),
        dma((2, PARTS, chips)),
        dma((2, PARTS, chips)),
        dma((2, PARTS, chips)),
        dma((2, PARTS, chips)),
        dma((2, PARTS, chips)),
        dma((2, PARTS, chips)),
        dma((2, PARTS, chips)),
        dma((2, PARTS, chips)),
        dma((PARTS, 4)),
        dma((PARTS, 4)),
    ]
    return pl.pallas_call(
        functools.partial(kernel, chips),
        out_shape=jax.ShapeDtypeStruct(tokens.shape, bf16),
        in_specs=[vmem] * 10 + [anywhere] * 6,
        out_specs=vmem,
        scratch_shapes=scratch,
        compiler_params=pltpu.CompilerParams(
            collective_id=0, has_side_effects=True, vmem_limit_bytes=62 * 2**20
        ),
    )(
        tokens,
        row(gain_first),
        row(down_first_scale),
        row(gain_second),
        row(down_second_scale),
        row(gain_last),
        gate_first_scale,
        up_first_scale,
        gate_second_scale,
        up_second_scale,
        gate_first,
        up_first,
        down_first,
        gate_second,
        up_second,
        down_second,
    )


def plan_for(mesh):
    ra, cb = mesh.shape["ra"], mesh.shape["cb"]

    def run(tokens, *rest):
        units = rest[1].shape[1]
        aligned = units % (cb * 8) == 0 and units % 128 == 0 and tokens.shape[0] % (32 * PARTS) == 0
        if ra == 4 and cb == 8 and aligned:
            return fused(tokens, *rest)
        return shards(tokens, *rest)

    return run


def solution(mesh):
    placed = (
        P("cb", "ra"),
        P(),
        P("cb", "ra"),
        P("ra"),
        P("cb", "ra"),
        P("ra"),
        P("ra", "cb"),
        P(),
        P(),
        P("cb", "ra"),
        P("ra"),
        P("cb", "ra"),
        P("ra"),
        P("ra", "cb"),
        P(),
        P(),
    )
    return jax.shard_map(
        plan_for(mesh), mesh=mesh, in_specs=placed, out_specs=P("cb", "ra"), check_vma=False
    )
```

```python
import functools

import jax
import jax.numpy as jnp
from jax import lax
from jax.experimental import pallas as pl
from jax.experimental.pallas import tpu as pltpu
from jax.sharding import PartitionSpec as P

MESH = pl.DeviceIdType.MESH
PARTS = 2
D = 2048


def own_slice(vector, width):
    return lax.dynamic_slice_in_dim(vector, lax.axis_index("ra") * width, width, 0)


def full_norm(values, gain):
    meansq = jnp.mean(values * values, axis=1, keepdims=True)
    return (values * lax.rsqrt(meansq + 1e-06) * gain).astype(jnp.bfloat16)


def expand(normed, w_gate, s_gate, w_up, s_up, w_down):
    gate = jnp.dot(
        normed,
        lax.all_gather(w_gate.astype(jnp.bfloat16), "cb", axis=0, tiled=True),
        preferred_element_type=jnp.float32,
    )
    upper = jnp.dot(
        normed,
        lax.all_gather(w_up.astype(jnp.bfloat16), "cb", axis=0, tiled=True),
        preferred_element_type=jnp.float32,
    )
    hidden = (jax.nn.silu(gate * s_gate) * (upper * s_up)).astype(jnp.bfloat16)
    return jnp.dot(
        hidden,
        lax.all_gather(w_down.astype(jnp.bfloat16), "cb", axis=1, tiled=True),
        preferred_element_type=jnp.float32,
    )


def reduce_share(partial_value):
    return lax.psum_scatter(
        partial_value.astype(jnp.bfloat16), "ra", scatter_dimension=1, tiled=True
    ).astype(jnp.float32)


def shards(
    tokens,
    gain_first,
    gate_first,
    gate_first_scale,
    up_first,
    up_first_scale,
    down_first,
    down_first_scale,
    gain_second,
    gate_second,
    gate_second_scale,
    up_second,
    up_second_scale,
    down_second,
    down_second_scale,
    gain_last,
):
    width = tokens.shape[1]
    whole_in = lax.all_gather(tokens, "ra", axis=1, tiled=True).astype(jnp.float32)
    normed = full_norm(whole_in, gain_first)
    partial_value = expand(
        normed, gate_first, gate_first_scale, up_first, up_first_scale, down_first
    )
    summed = lax.psum(partial_value.astype(jnp.bfloat16), "ra").astype(jnp.float32)
    first = 0.1 * whole_in + 0.5 * summed * down_first_scale
    first_share = own_slice(first.T, width).T
    normed_next = full_norm(first, gain_second)
    partial_next = expand(
        normed_next, gate_second, gate_second_scale, up_second, up_second_scale, down_second
    )
    second = 0.1 * first_share + 0.5 * reduce_share(partial_next) * own_slice(
        down_second_scale, width
    )
    closing = lax.psum(jnp.sum(second * second, axis=1), "ra")
    return (second * lax.rsqrt(closing / D + 1e-06)[:, None] * own_slice(gain_last, width)).astype(
        jnp.bfloat16
    )


def remote(source, target, sent, received, device):
    return pltpu.make_async_remote_copy(
        src_ref=source,
        dst_ref=target,
        send_sem=sent,
        recv_sem=received,
        device_id=device,
        device_id_type=MESH,
    )


def kernel(chips, *refs):
    (tokens, gain_first, scale_first, gain_second, scale_second, gain_last) = refs[:6]
    scales = refs[6:10]
    weights = refs[10:16]
    out = refs[16]
    stages = refs[17:23]
    (
        sendable,
        whole,
        rows_in,
        normed,
        hidden,
        product,
        given,
        taken,
        passed,
        from_below,
        from_above,
        total,
        first,
        stats,
        last,
        vectors,
        load_sem,
        wz_s,
        wz_r,
        wp_s,
        wp_r,
        wk_s,
        wk_r,
        tx_s,
        tx_r,
        az_s,
        az_r,
        ay_s,
        ay_r,
        ry_s,
        ry_r,
        rz_s,
        rzu_r,
        rzd_r,
        end_s,
        end_r,
    ) = refs[23:]
    count = chips
    half_rows = tokens.shape[0] // 2
    columns = tokens.shape[1]
    width = 4 * columns
    half = width // 2
    units = sendable.shape[1]
    share = units // count
    part_rows = half_rows // PARTS
    piece = sendable.shape[2]

    ra, cb = lax.axis_index("ra"), lax.axis_index("cb")
    y, x = lax.div(ra, 2), lax.rem(ra, 2)
    z, k = lax.div(cb, 2), lax.rem(cb, 2)
    p, q = x + k * (y - x), y + k * (x - y)
    far = lax.div(z, 2)

    def device(x_at, y_at, z_at, k_at):
        return (y_at * 2 + x_at, z_at * 2 + k_at)

    def turned(p_at, q_at):
        return device(p_at + k * (q_at - p_at), q_at + k * (p_at - q_at), z, k)

    on_p, on_q = turned(1 - p, q), turned(p, 1 - q)
    on_k = device(x, y, z, 1 - k)
    to_x, to_y = device(1 - x, y, z, 0), device(x, 1 - y, z, 1)
    above = device(x, y, lax.rem(z + 1, count), k)
    below = device(x, y, lax.rem(z + count - 1, count), k)

    def around(d):
        return lax.rem(z + d, count)

    def near(i):
        outer, inner = i // 2, i % 2
        close = z + inner * (1 - 2 * lax.rem(z, 2))
        distant = (2 + inner) - far * (1 + 2 * inner)
        return (1 - outer) * close + outer * distant

    def natural(block):
        return block if block in (0, 3) else (1 + k if block == 1 else 2 - k)

    def at_share(n):
        return pl.ds(pl.multiple_of(n * share, 16), share)

    def at_column(z_at, k_at):
        return pl.ds(pl.multiple_of(k_at * half + z_at * piece, 128), piece)

    def at_half(h):
        return pl.ds(pl.multiple_of(h * half, 128), half)

    def at_block(n):
        return pl.ds(pl.multiple_of(n * columns, 128), columns)

    sends = []

    def launch(copy):
        copy.start()
        sends.append((None, copy))

    def launch_if(condition, copy):
        @pl.when(condition)
        def _():
            copy.start()

        sends.append((condition, copy))

    barrier = pltpu.get_barrier_semaphore()
    partners = [device(1 - x, y, z, 0), device(1 - x, y, z, 1), device(x, 1 - y, z, 0)]
    partners += [device(x, 1 - y, z, 1), device(1 - x, 1 - y, z, k), on_k]
    partners += [device(x, y, around(d), k) for d in range(1, count)]
    for partner in partners:
        pl.semaphore_signal(barrier, inc=1, device_id=partner, device_id_type=MESH)
    loads = [
        pltpu.make_async_copy(weights[m], stages[m], load_sem.at[m]) for m in range(6)
    ]
    for load in loads:
        load.start()
    for n, vector in enumerate((gain_first, scale_first, gain_second, scale_second, gain_last)):
        for block in range(4):
            vectors[n, :, block * columns : (block + 1) * columns] = vector[
                :, at_block(natural(block))
            ]

    def prepare(m):
        loads[m].wait()
        if m % 3 == 2:
            sendable[m] = stages[m][...].astype(jnp.bfloat16)
        else:
            scale = scales[2 * (m // 3) + m % 3]
            for at in range(0, units, 128):
                block = stages[m][:, at : at + 128] * scale[at : at + 128][None, :]
                sendable[m, at : at + 128, :] = block.T.astype(jnp.bfloat16)
        whole[m, at_share(p), at_column(z, k)] = sendable[m, at_share(z), :]

    def z_copy(m, d):
        return remote(
            sendable.at[m, at_share(around(d)), :],
            whole.at[m, at_share(p), at_column(z, k)],
            wz_s.at[m, d - 1],
            wz_r.at[m, d - 1],
            device(x, y, around(d), k),
        )

    odd = lax.rem(z, 2)
    outgoing = {"across": 2, "beyond": 3 - 2 * odd, "beside": 1 + 2 * odd}
    incoming = {"own": 0, "across": 2, "beyond": 1 + 2 * odd, "beside": 3 - 2 * odd}

    def send_z(m, *steps):
        for step in steps:
            launch(z_copy(m, outgoing[step]))

    def relay(m, *steps):
        for step in steps:
            d = incoming[step]
            place = at_column(around(count - d), k)
            if step != "own":
                z_copy(m, d).wait_recv()
                source = whole.at[m, at_share(p), place]
            else:
                source = sendable.at[m, at_share(z), :]
            remote(
                source, whole.at[m, at_share(x), place], wp_s.at[m, 0], wp_r.at[m], to_x
            ).start()
            remote(
                source, whole.at[m, at_share(y), place], wp_s.at[m, 1], wp_r.at[m], to_y
            ).start()
            remote(
                source, whole.at[m, at_share(q), place], wk_s.at[m], wk_r.at[m], on_k
            ).start()

    def await_weights(m):
        part = whole.at[m, at_share(1 - p), :]
        remote(part, part, wp_s.at[m, 0], wp_r.at[m], on_p).wait_recv()
        part = whole.at[m, at_share(p), at_half(1 - k)]
        remote(part, part, wk_s.at[m], wk_r.at[m], on_k).wait_recv()

    def drain_weights(m):
        part = whole.at[m, at_share(p), at_half(k)]
        remote(part, part, wp_s.at[m, 0], wp_r.at[m], to_x).wait_send()
        remote(part, part, wp_s.at[m, 1], wp_r.at[m], to_y).wait_send()
        remote(part, part, wk_s.at[m], wk_r.at[m], on_k).wait_send()

    def rows_of(h):
        return slice(h * part_rows, (h + 1) * part_rows)

    def gather_z(b, i, h, up):
        j = near(i)
        part = rows_in.at[b, j, rows_of(h), at_half(q)]
        return remote(
            part,
            part,
            az_s.at[b, h, i + (0 if up or i else count)],
            az_r.at[b, h, j],
            above if up else below,
        )

    def gather_q(b, i, h):
        part = rows_in.at[b, near(i), rows_of(h), at_half(q)]
        return remote(part, part, ay_s.at[b, h, i], ay_r.at[b, h, i], on_q)

    def gather_step(b, i, h):
        j = near(i)
        if i == 0:
            launch_if(z < count - 1, gather_z(b, 0, h, True))
            launch_if(z > 0, gather_z(b, 0, h, False))
        else:
            gather_z(b, i, h, True).wait_recv()
            launch_if((j < z) & (z < count - 1), gather_z(b, i, h, True))
            launch_if((j > z) & (z > 0), gather_z(b, i, h, False))
        launch(gather_q(b, i, h))

    def norm_step(b, i):
        j = near(i)
        for h in range(PARTS):
            gather_q(b, i, h).wait_recv()
        values = rows_in[b, j].astype(jnp.float32)
        meansq = jnp.sum(values * values, axis=1, keepdims=True) * (1.0 / width)
        values = values * lax.rsqrt(meansq + 1e-06) * vectors[2 * b]
        values = values.astype(jnp.bfloat16)
        rows = slice(i * half_rows, (i + 1) * half_rows)
        for block in range(4):
            for side in range(2):
                at = block * columns + side * piece
                normed[rows, at_column(natural(block), side)] = values[:, at : at + piece]

    def expand_step(b, pair):
        axes = (((1,), (1,)), ((), ()))
        rows = pl.ds(pl.multiple_of(pair * 2 * half_rows, 16), 2 * half_rows)
        gate = lax.dot_general(
            normed[rows, :], whole[3 * b], axes, preferred_element_type=jnp.float32
        )
        upper = lax.dot_general(
            normed[rows, :], whole[3 * b + 1], axes, preferred_element_type=jnp.float32
        )
        hidden[rows, :] = (gate / (1.0 + jnp.exp(-gate)) * upper).astype(jnp.bfloat16)

    def reduce_q(b, i, h):
        j = near(i)
        return remote(
            given.at[b, j, rows_of(h)],
            taken.at[b, j, rows_of(h)],
            ry_s.at[b, h, i],
            ry_r.at[b, h, i],
            on_q,
        )

    def contract_step(b, i):
        j = near(i)
        rows = pl.ds(pl.multiple_of(i * half_rows, 16), half_rows)
        for side in range(2):
            part = jnp.dot(
                hidden[rows, :],
                whole[3 * b + 2, :, side * half : (side + 1) * half],
                preferred_element_type=jnp.float32,
            )
            for block in range(4):
                at = pl.multiple_of(natural(block) * columns + side * piece, 128)
                product[j, :, pl.ds(at, piece)] = part[:, block * piece : (block + 1) * piece]
        given[b, j] = product[j, :, at_half(1 - q)].astype(jnp.bfloat16)
        for h in range(PARTS):
            reduce_q(b, i, h).start()

    def reduce_z(b, i, h, up):
        j = near(i)
        landing, arrived, target = (
            (from_below, rzu_r, above) if up else (from_above, rzd_r, below)
        )
        return remote(
            passed.at[b, j, rows_of(h)],
            landing.at[b, j, rows_of(h)],
            rz_s.at[b, h, i],
            arrived.at[b, h, j],
            target,
        )

    def reduce_step(b, i, h):
        j = near(i)
        rows = rows_of(h)
        reduce_q(b, i, h).wait_recv()
        total[rows] = product[j, rows, at_half(q)] + taken[b, j, rows].astype(jnp.float32)
        rises = (j >= z) & (z > 0)
        falls = (j <= z) & (z < count - 1)

        @pl.when(rises)
        def _():
            reduce_z(b, i, h, True).wait_recv()
            total[rows] += from_below[b, j, rows].astype(jnp.float32)

        @pl.when(falls)
        def _():
            reduce_z(b, i, h, False).wait_recv()
            total[rows] += from_above[b, j, rows].astype(jnp.float32)

        if i:
            passed[b, j, rows] = total[rows].astype(jnp.bfloat16)
            launch_if(j > z, reduce_z(b, i, h, True))
            launch_if(j < z, reduce_z(b, i, h, False))

    def restart(h):
        rows = rows_of(h)
        start = rows_in[0, z, rows, at_half(q)].astype(jnp.float32)
        first[rows] = 0.1 * start + 0.5 * total[rows] * vectors[1, :, at_half(q)]
        rows_in[1, z, rows, at_half(q)] = first[rows].astype(jnp.bfloat16)

    gains = vectors[4, :, at_block(2 * q + p)]

    def settle(copies):
        for condition, copy in copies:
            if condition is None:
                copy.wait_send()
            else:

                @pl.when(condition)
                def _(copy=copy):
                    copy.wait_send()

    def settle_early(copies):
        settle(copies)
        for m in range(6):
            drain_weights(m)
        for i in range(count):
            for h in range(PARTS):
                reduce_q(0, i, h).wait_send()

    def end_copies(h):
        copies = [
            remote(stats.at[0, h], stats.at[1 + n, h], end_s.at[h, n], end_r.at[h, n], target)
            for n, target in enumerate((on_q, on_p, turned(1 - p, 1 - q)))
        ]
        part = rows_of(h)
        copies.append(
            remote(last.at[0, part], last.at[1, part], end_s.at[h, 3], end_r.at[h, 3], on_p)
        )
        return copies

    def spread(n, h):
        return jnp.broadcast_to(stats[n, h][:1], (128, part_rows)).T[:, :1]

    def end_step(h):
        rows = rows_of(h)
        total[rows] = 0.1 * first[rows] + 0.5 * total[rows] * vectors[3, :, at_half(q)]
        squares = jnp.sum(total[rows] * total[rows], axis=1, keepdims=True)
        stats[0, h] = jnp.broadcast_to(squares, (part_rows, 128)).T[:8]
        last[0, rows] = total[rows, at_block(1 - p)].astype(jnp.bfloat16)
        for copy in end_copies(h):
            launch(copy)

    def finish_step(h):
        rows = rows_of(h)
        copies = end_copies(h)
        copies[0].wait_recv()
        factor = lax.rsqrt((spread(0, h) + spread(1, h)) * (1.0 / width) + 1e-06)
        own = pl.ds(pl.multiple_of(p * half_rows + h * part_rows, 16), part_rows)
        out[own, :] = (total[rows, at_block(p)] * factor * gains).astype(jnp.bfloat16)
        for copy in copies[1:]:
            copy.wait_recv()
        factor = lax.rsqrt((spread(2, h) + spread(3, h)) * (1.0 / width) + 1e-06)
        other = pl.ds(pl.multiple_of((1 - p) * half_rows + h * part_rows, 16), part_rows)
        out[other, :] = (last[1, rows].astype(jnp.float32) * factor * gains).astype(jnp.bfloat16)

    prepare(0)
    pl.semaphore_wait(barrier, len(partners))

    mine = pl.ds(pl.multiple_of(p * half_rows, 16), half_rows)
    theirs = pl.ds(pl.multiple_of((1 - p) * half_rows, 16), half_rows)
    own_columns = at_block(2 * q + p)
    token_copies = [
        remote(
            tokens.at[
                pl.ds(pl.multiple_of((1 - p) * half_rows + h * part_rows, 16), part_rows), :
            ],
            rows_in.at[0, z, rows_of(h), own_columns],
            tx_s.at[h],
            tx_r.at[h],
            on_p,
        )
        for h in range(PARTS)
    ]
    for copy in token_copies:
        launch(copy)
    send_z(0, "across")
    rows_in[0, z, :, own_columns] = tokens[mine, :]
    prepare(1)
    for h in range(PARTS):
        token_copies[h].wait_recv()
        gather_step(0, 0, h)
    send_z(0, "beside")
    relay(0, "own")
    prepare(2)
    prepare(3)
    prepare(4)
    prepare(5)
    gather_step(0, 1, 0)
    gather_step(0, 1, 1)
    send_z(0, "beyond")
    send_z(1, "across", "beyond")
    relay(0, "across")
    relay(1, "own")
    gather_step(0, 2, 0)
    gather_step(0, 2, 1)
    send_z(1, "beside")
    send_z(2, "across")
    relay(0, "beside")
    gather_step(0, 3, 0)
    gather_step(0, 3, 1)
    send_z(2, "beyond", "beside")
    relay(0, "beyond")
    relay(1, "across")
    norm_step(0, 0)
    norm_step(0, 1)
    send_z(3, "across", "beyond", "beside")
    relay(1, "beyond")
    norm_step(0, 2)
    norm_step(0, 3)
    relay(1, "beside")
    relay(2, "own", "across", "beyond", "beside")
    send_z(4, "across", "beyond", "beside")
    await_weights(0)
    await_weights(1)
    lax.fori_loop(0, 2, lambda i, c: (expand_step(0, i), c)[1], 0)
    await_weights(2)
    lax.fori_loop(0, count, lambda i, c: (contract_step(0, count - 1 - i), c)[1], 0)
    reduce_step(0, 3, 0)
    reduce_step(0, 3, 1)
    relay(3, "own", "across")
    reduce_step(0, 2, 0)
    reduce_step(0, 2, 1)
    relay(3, "beyond")
    reduce_step(0, 1, 0)
    reduce_step(0, 1, 1)
    relay(3, "beside")
    relay(4, "own")
    reduce_step(0, 0, 0)
    restart(0)
    gather_step(1, 0, 0)
    reduce_step(0, 0, 1)
    restart(1)
    gather_step(1, 0, 1)
    relay(4, "across")
    gather_step(1, 1, 0)
    gather_step(1, 1, 1)
    relay(4, "beyond")
    send_z(5, "across")
    gather_step(1, 2, 0)
    gather_step(1, 2, 1)
    relay(4, "beside")
    send_z(5, "beyond")
    gather_step(1, 3, 0)
    gather_step(1, 3, 1)
    send_z(5, "beside")
    relay(5, "own", "across")
    norm_step(1, 0)
    norm_step(1, 1)
    norm_step(1, 2)
    norm_step(1, 3)
    await_weights(3)
    await_weights(4)
    relay(5, "beyond")
    lax.fori_loop(0, 2, lambda i, c: (expand_step(1, i), c)[1], 0)
    relay(5, "beside")
    await_weights(5)
    settled = len(sends)
    lax.fori_loop(0, count, lambda i, c: (contract_step(1, count - 1 - i), c)[1], 0)
    reduce_step(1, 3, 0)
    reduce_step(1, 3, 1)
    reduce_step(1, 2, 0)
    reduce_step(1, 2, 1)
    reduce_step(1, 1, 0)
    reduce_step(1, 1, 1)
    settle_early(sends[:settled])
    reduce_step(1, 0, 0)
    end_step(0)
    reduce_step(1, 0, 1)
    end_step(1)
    finish_step(0)
    finish_step(1)
    for i in range(count):
        for h in range(PARTS):
            reduce_q(1, i, h).wait_send()
    settle(sends[settled:])


def fused(tokens, *rest):
    (
        gain_first,
        gate_first,
        gate_first_scale,
        up_first,
        up_first_scale,
        down_first,
        down_first_scale,
        gain_second,
        gate_second,
        gate_second_scale,
        up_second,
        up_second_scale,
        down_second,
        down_second_scale,
        gain_last,
    ) = rest
    chips = lax.axis_size("cb") // 2
    rows, columns = tokens.shape
    piece, units = gate_first.shape
    share = units // chips
    width, half_rows = 4 * columns, rows // 2
    half = width // 2

    def row(vector):
        return vector.reshape(1, -1)

    vmem = pl.BlockSpec(memory_space=pltpu.VMEM)
    anywhere = pl.BlockSpec(memory_space=pl.ANY)
    bf16, f32 = jnp.bfloat16, jnp.float32
    dma = pltpu.SemaphoreType.DMA
    stage_shapes = [w.shape for w in (gate_first, up_first, down_first)] * 2
    moved = pltpu.VMEM((2, chips, half_rows, half), bf16)
    scratch = [pltpu.VMEM(shape, f32) for shape in stage_shapes] + [
        pltpu.VMEM((6, units, piece), bf16),
        pltpu.VMEM((6, 2 * share, width), bf16),
        pltpu.VMEM((2, chips, half_rows, width), bf16),
        pltpu.VMEM((chips * half_rows, width), bf16),
        pltpu.VMEM((chips * half_rows, 2 * share), bf16),
        pltpu.VMEM((chips, half_rows, width), f32),
        moved,
        moved,
        moved,
        moved,
        moved,
        pltpu.VMEM((half_rows, half), f32),
        pltpu.VMEM((half_rows, half), f32),
        pltpu.VMEM((4, PARTS, 8, half_rows // PARTS), f32),
        pltpu.VMEM((2, half_rows, columns), bf16),
        pltpu.VMEM((5, 1, width), f32),
        dma((6,)),
        dma((6, chips - 1)),
        dma((6, chips - 1)),
        dma((6, 2)),
        dma((6,)),
        dma((6,)),
        dma((6,)),
        dma((PARTS,)),
        dma((PARTS,)),
        dma((2, PARTS, chips + 1)),
        dma((2, PARTS, chips)),
        dma((2, PARTS, chips)),
        dma((2, PARTS, chips)),
        dma((2, PARTS, chips)),
        dma((2, PARTS, chips)),
        dma((2, PARTS, chips)),
        dma((2, PARTS, chips)),
        dma((2, PARTS, chips)),
        dma((PARTS, 4)),
        dma((PARTS, 4)),
    ]
    return pl.pallas_call(
        functools.partial(kernel, chips),
        out_shape=jax.ShapeDtypeStruct(tokens.shape, bf16),
        in_specs=[vmem] * 10 + [anywhere] * 6,
        out_specs=vmem,
        scratch_shapes=scratch,
        compiler_params=pltpu.CompilerParams(
            collective_id=0, has_side_effects=True, vmem_limit_bytes=62 * 2**20
        ),
    )(
        tokens,
        row(gain_first),
        row(down_first_scale),
        row(gain_second),
        row(down_second_scale),
        row(gain_last),
        gate_first_scale,
        up_first_scale,
        gate_second_scale,
        up_second_scale,
        gate_first,
        up_first,
        down_first,
        gate_second,
        up_second,
        down_second,
    )


def plan_for(mesh):
    ra, cb = mesh.shape["ra"], mesh.shape["cb"]

    def run(tokens, *rest):
        units = rest[1].shape[1]
        aligned = units % (cb * 8) == 0 and units % 128 == 0 and tokens.shape[0] % (32 * PARTS) == 0
        if ra == 4 and cb == 8 and aligned:
            return fused(tokens, *rest)
        return shards(tokens, *rest)

    return run


def solution(mesh):
    placed = (
        P("cb", "ra"),
        P(),
        P("cb", "ra"),
        P("ra"),
        P("cb", "ra"),
        P("ra"),
        P("ra", "cb"),
        P(),
        P(),
        P("cb", "ra"),
        P("ra"),
        P("cb", "ra"),
        P("ra"),
        P("ra", "cb"),
        P(),
        P(),
    )
    return jax.shard_map(
        plan_for(mesh), mesh=mesh, in_specs=placed, out_specs=P("cb", "ra"), check_vma=False
    )
```
